32 devices in a mesh: tp: 32 (over z, y, x, core).
Axes of the slice: x: 2, y: 2, z: 4, core: 2. Of those that a mesh axis runs over, the one named last changes fastest.
Arguments:
- stream: bfloat16 [1024, 2048], P('tp'), may hold values from -15 to 15
- norm_gain: bfloat16 [4096], replicated, may hold values from 0.099609375 to 1.8984375
- query_weight: bfloat16 [65536, 128], P('tp'), may hold values from -0.09375 to 0.09375
- key_weight: bfloat16 [65536, 128], P('tp'), may hold values from -0.09375 to 0.09375
- value_weight: bfloat16 [65536, 128], P('tp'), may hold values from -0.09375 to 0.09375
- gate_weight: bfloat16 [65536, 128], P('tp'), may hold values from -0.09375 to 0.09375
- write_weight: bfloat16 [4096, 16], replicated, may hold values from -0.09375 to 0.09375
- decay_weight: bfloat16 [4096, 16], replicated, may hold values from -0.09375 to 0.09375
- decay_rate: float32 [16], replicated, may hold values from 0.02 to 2
- head_gain: bfloat16 [128], replicated, may hold values from 0.099609375 to 1.8984375
- out_weight: bfloat16 [65536, 128], P('tp'), may hold values from -0.125 to 0.125
- state: float32 [8192, 128, 128], P('tp'), may hold values from -4 to 4
Outputs:
- stream_out: bfloat16 [1024, 2048], P('tp')
- state_out: float32 [8192, 128, 128], P('tp')
The draws below stay inside these ranges and needn't reach their ends.
All inputs are finite; a program needn't handle non-finite values.
Results may differ from the reference program's by a relative error of at most 0.012.
Values may be sent and summed in bfloat16 or wider, within the bound.
A program may use at most 128 MiB of HBM per device.

```python
import math
import jax
import jax.numpy as jnp
from jax import lax

D = 4096
H = 16
DK = 128
BATCH = 512
SEQ_GROUPS = 2
DG = 2048
BG = 256


def draw_stream(key, part):
    key_vals, key_scales = jax.random.split(jax.random.fold_in(key, 17))
    values = jnp.clip(jax.random.normal(key_vals, (BATCH, D), jnp.float32), -5.0, 5.0)
    scales = jnp.exp(jax.random.uniform(key_scales, (D // 128,), jnp.float32, jnp.log(0.3), jnp.log(3.0)))
    whole = values * jnp.repeat(scales, 128)[None, :]
    return whole.reshape(BATCH, SEQ_GROUPS, DG).transpose(1, 0, 2).reshape(SEQ_GROUPS * BATCH, DG).astype(jnp.bfloat16)


def level_of(stream_key, shape, pieces, smallest, top_value):
    loudness, own = 1.0, jax.random.fold_in(stream_key, 6)
    for dim, parts in pieces:
        draws = jnp.exp(jax.random.uniform(jax.random.fold_in(own, dim), (parts,), jnp.float32, smallest / len(pieces), top_value / len(pieces)))
        loudness = loudness * jnp.repeat(draws, shape[dim] // parts).reshape([-1 if axis == dim else 1 for axis in range(len(shape))])
    return loudness


def noise(stream_key, shape, spread, bound, cuts=(), dtype=jnp.bfloat16):
    values = spread * jax.random.normal(stream_key, shape, jnp.float32)
    if cuts:
        values = values * level_of(stream_key, shape, cuts, -0.22, 0.18)
    return jnp.clip(values, -bound, bound).astype(dtype)


def setup_inputs(seed: int = 0) -> dict:
    key_list = jax.random.split(jax.random.key(seed), 13)
    return {
        "stream": draw_stream(jax.random.fold_in(key_list[12], 71), 0),
        "norm_gain": jnp.clip(1.0 + 0.18 * jax.random.normal(key_list[1], (D,), jnp.float32), 0.099609375, 1.8984375).astype(jnp.bfloat16),
        "query_weight": noise(key_list[2], (H * D, DK), D ** -0.5, 0.09375, ((0, 32),)),
        "key_weight": noise(key_list[3], (H * D, DK), D ** -0.5, 0.09375, ((0, 32),)),
        "value_weight": noise(key_list[4], (H * D, DK), D ** -0.5, 0.09375, ((0, 32),)),
        "gate_weight": noise(key_list[5], (H * D, DK), D ** -0.5, 0.09375, ((0, 32),)),
        "write_weight": noise(key_list[6], (D, H), D ** -0.5, 0.09375),
        "decay_weight": noise(key_list[7], (D, H), D ** -0.5, 0.09375),
        "decay_rate": jnp.clip(jnp.exp(jax.random.uniform(key_list[8], (H,), jnp.float32, math.log(0.02), math.log(2.0))), 0.02, 2.0),
        "head_gain": jnp.clip(1.0 + 0.18 * jax.random.normal(key_list[9], (DK,), jnp.float32), 0.099609375, 1.8984375).astype(jnp.bfloat16),
        "out_weight": noise(key_list[10], (H * D, DK), (H * DK) ** -0.5, 0.125, ((0, 32),)),
        "state": noise(key_list[11], (BATCH * H, DK, DK), 0.5, 4.0, ((0, 32),), jnp.float32),
    }


EPS = 1e-06

def reference(stream, norm_gain, query_weight, key_weight, value_weight, gate_weight, write_weight, decay_weight, decay_rate, head_gain, out_weight, state):
    highest = lax.Precision.HIGHEST
    stream_f = stream.reshape(SEQ_GROUPS, BATCH, DG).transpose(1, 0, 2).reshape(BATCH, D).astype(jnp.float32)
    gained = (stream_f * norm_gain.astype(jnp.float32)).astype(jnp.bfloat16)
    row_scale = lax.rsqrt(lax.optimization_barrier(jnp.mean(stream_f * stream_f, axis=-1)) + EPS)

    def logical(weight):
        return weight.reshape(SEQ_GROUPS, H, DG, DK).transpose(0, 2, 1, 3).reshape(D, H * DK)

    def project(weight):
        product = jnp.dot(gained, weight, preferred_element_type=jnp.float32)
        return (product * row_scale[:, None]).astype(jnp.bfloat16).astype(jnp.float32)
    query_raw = project(logical(query_weight)).reshape(BATCH, H, DK)
    key_raw = project(logical(key_weight)).reshape(BATCH, H, DK)
    value_vec = project(logical(value_weight)).reshape(BATCH, H, DK)
    gate_vec = project(logical(gate_weight)).reshape(BATCH, H, DK)
    write_pre = project(write_weight)
    decay_pre = project(decay_weight)
    query_vec = query_raw * lax.rsqrt(lax.optimization_barrier(jnp.sum(query_raw * query_raw, axis=-1, keepdims=True)) + EPS) * DK ** (-0.5)
    key_vec = key_raw * lax.rsqrt(lax.optimization_barrier(jnp.sum(key_raw * key_raw, axis=-1, keepdims=True)) + EPS)
    strength = jax.nn.sigmoid(write_pre)
    decay_factor = jnp.exp(-decay_rate[None, :] * jax.nn.softplus(decay_pre))
    memory = state.reshape(SEQ_GROUPS, H, BG, DK, DK).transpose(0, 2, 1, 3, 4).reshape(BATCH, H, DK, DK)
    recalled = jnp.einsum('bhdj,bhd->bhj', memory, key_vec, precision=highest)
    correction = strength[..., None] * (value_vec - decay_factor[..., None] * recalled)
    updated = decay_factor[..., None, None] * memory + key_vec[..., :, None] * correction[..., None, :]
    readout = jnp.einsum('bhdj,bhd->bhj', updated, query_vec, precision=highest)
    scaling = lax.rsqrt(lax.optimization_barrier(jnp.mean(readout * readout, axis=-1)) + EPS)
    gated_rows = (readout * head_gain.astype(jnp.float32) * jax.nn.silu(gate_vec)).astype(jnp.bfloat16)
    out_heads = out_weight.reshape(SEQ_GROUPS, H, DG, DK).transpose(1, 3, 0, 2).reshape(H, DK, D)
    head_sums = jnp.zeros((BATCH, D), jnp.float32)
    for head_index in range(H):
        term = jnp.dot(gated_rows[:, head_index], out_heads[head_index], preferred_element_type=jnp.float32)
        head_sums = head_sums + term * scaling[:, head_index, None]
    result = (stream_f + head_sums).astype(jnp.bfloat16)
    stream_out = result.reshape(BATCH, SEQ_GROUPS, DG).transpose(1, 0, 2).reshape(SEQ_GROUPS * BATCH, DG)
    state_out = updated.reshape(SEQ_GROUPS, BG, H, DK, DK).transpose(0, 2, 1, 3, 4).reshape(BATCH * H, DK, DK)
    return (stream_out, state_out)
```

```python
import functools

import jax
import jax.numpy as jnp
from jax import lax
from jax.experimental import pallas as pl
from jax.experimental.pallas import tpu as pltpu
from jax.sharding import PartitionSpec as P

EPS = 1e-06
MESH = pl.DeviceIdType.MESH
VMEM = pl.BlockSpec(memory_space=pltpu.VMEM)
SMALL = 16


def flip(me, bits):
    other = me
    for bit in bits:
        other = other + (1 - 2 * ((me // (1 << bit)) % 2)) * (1 << bit)
    return other


def parts_of(cols, dims):
    tiles = cols // 128
    count = max(1, min(dims, tiles))
    cuts = [tiles * i // count * 128 for i in range(count + 1)]
    ranges = [(cuts[i], cuts[i + 1] - cuts[i]) for i in range(count)]
    orders = [[1 + (i + j) % dims for j in range(dims)] for i in range(count)]
    return list(zip(ranges, orders))


def masks_of(order):
    sets = [((), -1)]
    for step in range(len(order)):
        sets = sets + [(bits + (order[step],), step) for bits, _ in sets]
    return sets


def key_of(bits):
    return sum(1 << (bit - 1) for bit in bits)


def enter(devices):
    barrier = pltpu.get_barrier_semaphore()
    for device in devices:
        pl.semaphore_signal(barrier, inc=1, device_id=(device,), device_id_type=MESH)
    pl.semaphore_wait(barrier, len(devices))


def remote(source, target, send_sem, recv_sem, device):
    return pltpu.make_async_remote_copy(
        src_ref=source,
        dst_ref=target,
        send_sem=send_sem,
        recv_sem=recv_sem,
        device_id=(device,),
        device_id_type=MESH,
    )


def project_kernel(
    heads,
    groups,
    stream_ref,
    gain_ref,
    query_w,
    key_w,
    value_w,
    gate_w,
    write_w,
    decay_w,
    rate_ref,
    packed_out,
    gathered,
    weights,
    write_t,
    decay_t,
    gains,
    local_sems,
    partial,
    sent,
    received,
    small_sent,
    small_received,
    turned,
    ici_send,
    ici_recv,
    core_send,
    core_recv,
    group_send,
    group_recv,
    small_send,
    small_recv,
):
    me = lax.axis_index("tp")
    place = me % heads
    group = me // heads
    rows, cols = stream_ref.shape
    batch = gathered.shape[0]
    group_rows = batch // groups
    dims = heads.bit_length() - 2
    sibling = flip(me, (0,))
    neighbours = [flip(me, (bit,)) for bit in range(1, dims + 1)]
    others = [place + heads * ((group + j) % groups) for j in range(1, groups)]
    size = query_w.shape[1]
    own_cols = pl.ds(pl.multiple_of(group * cols, cols), cols)
    fetches = [
        pltpu.make_async_copy(
            weight, weights.at[:, i * size : (i + 1) * size], local_sems.at[i]
        )
        for i, weight in enumerate((query_w, key_w, value_w, gate_w))
    ] + [
        pltpu.make_async_copy(source.at[:, own_cols], target, local_sems.at[4 + i])
        for i, (source, target) in enumerate(((write_w, write_t), (decay_w, decay_t)))
    ]
    for fetch in fetches:
        fetch.start()
    enter([sibling] + neighbours + others)

    halves = 2 if rows % 32 == 0 and group_rows % rows == 0 else 1
    part_rows = rows // halves
    half_batch = batch // halves
    ranges = parts_of(cols, dims)

    def half_rows(h, device_place):
        begin = h * half_batch + device_place * part_rows
        return pl.ds(pl.multiple_of(begin, part_rows), part_rows)

    def block(h, device_place, part):
        return gathered.at[half_rows(h, device_place), pl.ds(part[0][0], part[0][1])]

    sends = []
    core_copies = [[] for _ in range(halves)]

    def pass_on(h, p, part, bits, step):
        order = part[1]
        origin = flip(place, bits)
        target = block(h, origin, part)
        if bits:
            source = target
        else:
            source = stream_ref.at[
                pl.ds(h * part_rows, part_rows), pl.ds(part[0][0], part[0][1])
            ]
        for later in range(step + 1, dims):
            landed = key_of(bits + (order[later],))
            copy = remote(
                source,
                target,
                ici_send.at[h, p, landed],
                ici_recv.at[h, p, landed],
                flip(me, (order[later],)),
            )
            copy.start()
            sends.append(copy)
        own = key_of(bits)
        copy = remote(source, target, core_send.at[h, p, own], core_recv.at[h, p, own], sibling)
        copy.start()
        core_copies[h].append(copy)

    def begin(h):
        for p, part in enumerate(ranges):
            pass_on(h, p, part, (), -1)

    def relay(h, index):
        for p, part in enumerate(ranges):
            bits, step = masks_of(part[1])[index]
            landed = key_of(bits)
            target = block(h, flip(place, bits), part)
            remote(
                target, target, ici_send.at[h, p, landed], ici_recv.at[h, p, landed], sibling
            ).wait_recv()
            pass_on(h, p, part, bits, step)

    early = max(2, 1 << (dims - 1))
    begin(0)
    for h in range(halves):
        gathered[half_rows(h, place), :] = stream_ref[h * part_rows : (h + 1) * part_rows, :]
    relay(0, 1)
    for h in range(1, halves):
        begin(h)
    for index in range(2, 1 << dims):
        relay(0, index)
    for h in range(1, halves):
        for index in range(1, early):
            relay(h, index)
    for copy in core_copies[0]:
        copy.wait_recv()

    gains[...] = gain_ref[...].astype(jnp.float32)
    gain = jnp.concatenate(
        [gains[pl.ds(group * (cols // 128) + i, 1), :] for i in range(cols // 128)], axis=1
    )
    for fetch in fetches:
        fetch.wait()

    def project(begin, count, at):
        x = gathered[pl.ds(begin, count), :].astype(jnp.float32)
        gained = (x * gain).astype(jnp.bfloat16)
        partial[pl.ds(at, count), :] = jnp.dot(
            gained, weights[...], preferred_element_type=jnp.float32
        )
        mine = lax.broadcasted_iota(jnp.int32, (count, heads), 1) == place
        pre = [
            jnp.sum(
                jnp.where(
                    mine,
                    lax.dot_general(
                        gained,
                        w[...],
                        (((1,), (1,)), ((), ())),
                        preferred_element_type=jnp.float32,
                    ),
                    0.0,
                ),
                axis=1,
                keepdims=True,
            )
            for w in (write_t, decay_t)
        ]
        squares = jnp.sum(x * x, axis=1, keepdims=True)
        lane = lax.broadcasted_iota(jnp.int32, (count, 128), 1)
        return jnp.where(
            lane == 0, pre[0], jnp.where(lane == 1, pre[1], jnp.where(lane == 2, squares, 0.0))
        )

    copies = []
    wide = max(group_rows, 128)
    count = group_rows // halves

    def half_of(h, target_group):
        begin = h * half_batch + target_group * count
        return pl.multiple_of(begin, count)

    for h in range(halves):
        if h:
            for index in range(early, 1 << dims):
                relay(h, index)
            for copy in core_copies[h]:
                copy.wait_recv()
        for j in range(1, groups):
            spot = slice(h * count, (h + 1) * count)
            side = project(half_of(h, (group + j) % groups), count, 0)
            sent[j - 1, spot] = partial[0:count].astype(jnp.bfloat16)
            turned[spot] = side
            routes = [(sent.at[j - 1, spot], received.at[j - 1, spot], group_send, group_recv)]
            flat = turned[...].T
            small_sent[j - 1, :, spot] = flat[0:SMALL, spot].astype(jnp.bfloat16)
            routes.append(
                (
                    small_sent.at[j - 1, :, spot],
                    small_received.at[j - 1, :, spot],
                    small_send,
                    small_recv,
                )
            )
            for source, target, send, recv in routes:
                copy = remote(
                    source, target, send.at[h, j - 1], recv.at[h, j - 1], others[j - 1]
                )
                copy.start()
                copies.append(copy)
    for h in range(halves):
        turned[h * count : (h + 1) * count] = project(half_of(h, group), count, h * count)
    total = partial[...]
    flat = turned[...].T[0:SMALL, :]
    for copy in copies:
        copy.wait_recv()
    for j in range(1, groups):
        total = total + received[j - 1].astype(jnp.float32)
    small_total = flat[:, 0:group_rows]
    for j in range(1, groups):
        small_total = small_total + small_received[j - 1].astype(jnp.float32)
    turned_back = jnp.concatenate(
        [small_total, jnp.zeros((SMALL, wide - group_rows), jnp.float32)], axis=1
    ) if wide > group_rows else small_total
    side = jnp.concatenate(
        [turned_back, jnp.zeros((128 - SMALL, wide), jnp.float32)], axis=0
    ).T[0:group_rows]
    scale = lax.rsqrt(side[:, 2:3] / (cols * groups) + EPS)

    def rounded(v):
        return v.astype(jnp.bfloat16).astype(jnp.float32)

    projected = rounded(total * scale)
    query = projected[:, :size]
    key = projected[:, size : 2 * size]
    query = query * lax.rsqrt(jnp.sum(query * query, axis=1, keepdims=True) + EPS) * size**-0.5
    key = key * lax.rsqrt(jnp.sum(key * key, axis=1, keepdims=True) + EPS)
    pre = rounded(side * scale)
    strength = jax.nn.sigmoid(pre[:, 0:1])
    mine = lax.broadcasted_iota(jnp.int32, rate_ref.shape, 1) == place
    rate = jnp.sum(jnp.where(mine, rate_ref[...], 0.0), axis=1, keepdims=True)
    decay = pre[:, 1:2]
    softplus = jnp.maximum(decay, 0.0) + jnp.log(1.0 + jnp.exp(-jnp.abs(decay)))
    factor = jnp.exp(-rate * softplus)
    overlap = jnp.sum(query * key, axis=1, keepdims=True)
    results = [jnp.broadcast_to(v, (group_rows, size)) for v in (strength, factor, overlap)]
    results += [query, key, projected[:, 2 * size :]]
    for i, v in enumerate(results):
        span = pl.ds(i * size, v.shape[1])
        if halves == 1:
            packed_out[:, span] = v
            continue
        for h in range(halves):
            for q in range(group_rows // rows):
                to, come = q * rows + h * part_rows, h * count + q * part_rows
                packed_out[to : to + part_rows, span] = v[come : come + part_rows]
    for copy in sends + sum(core_copies, []) + copies:
        copy.wait_send()


def project(stream, norm_gain, weights, write_weight, decay_weight, rate, heads, groups):
    rows, cols = stream.shape
    batch = rows * heads
    group_rows = batch // groups
    size = weights[0].shape[1]
    dims = heads.bit_length() - 2
    parts = len(parts_of(cols, dims))
    extra = groups - 1
    halves = 2
    dma = pltpu.SemaphoreType.DMA
    anywhere = pl.BlockSpec(memory_space=pl.ANY)
    return pl.pallas_call(
        functools.partial(project_kernel, heads, groups),
        in_specs=[VMEM] * 2 + [anywhere] * 6 + [VMEM],
        out_specs=VMEM,
        out_shape=jax.ShapeDtypeStruct((group_rows, 7 * size), jnp.float32),
        scratch_shapes=[
            pltpu.VMEM((batch, cols), jnp.bfloat16),
            pltpu.VMEM((cols, 4 * size), jnp.bfloat16),
            pltpu.VMEM((heads, cols), jnp.bfloat16),
            pltpu.VMEM((heads, cols), jnp.bfloat16),
            pltpu.VMEM((groups * cols // 128, 128), jnp.float32),
            dma((6,)),
            pltpu.VMEM((group_rows, 4 * size), jnp.float32),
            pltpu.VMEM((extra, group_rows, 4 * size), jnp.bfloat16),
            pltpu.VMEM((extra, group_rows, 4 * size), jnp.bfloat16),
            pltpu.VMEM((extra, SMALL, group_rows), jnp.bfloat16),
            pltpu.VMEM((extra, SMALL, group_rows), jnp.bfloat16),
            pltpu.VMEM((max(group_rows, 128), 128), jnp.float32),
            dma((halves, parts, 1 << dims)),
            dma((halves, parts, 1 << dims)),
            dma((halves, parts, 1 << dims)),
            dma((halves, parts, 1 << dims)),
            dma((halves, extra)),
            dma((halves, extra)),
            dma((halves, extra)),
            dma((halves, extra)),
        ],
        compiler_params=pltpu.CompilerParams(
            collective_id=0, has_side_effects=True
        ),
    )(
        stream,
        norm_gain.reshape(groups * cols // 128, 128),
        *weights,
        write_weight.T,
        decay_weight.T,
        rate.reshape(1, heads),
    )


def split(v):
    high = v.astype(jnp.bfloat16)
    return high, (v - high.astype(jnp.float32)).astype(jnp.bfloat16)


def state_kernel(
    state_ref, packed_ref, gain_ref, new_ref, gated_ref, flat_ref, held, readout, in_sems, out_sems
):
    total, size, _ = state_ref.shape
    steps = in_sems.shape[0]
    count = total // steps

    def rows_of(step):
        return pl.ds(pl.multiple_of(step * count, count), count)

    def fetch(step):
        rows = rows_of(step)
        return pltpu.make_async_copy(state_ref.at[rows], held.at[rows], in_sems.at[step])

    def store(step):
        rows = rows_of(step)
        return pltpu.make_async_copy(held.at[rows], new_ref.at[rows], out_sems.at[step])

    for step in range(steps):
        fetch(step).start()
    spots = lax.broadcasted_iota(jnp.int32, (4 * count, size), 0) % count

    def diagonal(rows):
        marks = spots[0 : rows.shape[0]]
        return jnp.concatenate(
            [jnp.where(marks == b, rows, jnp.zeros_like(rows)) for b in range(count)], axis=1
        )

    def body(step, carry):
        rows = rows_of(step)

        def columns(first, width=1):
            return packed_ref[rows, first * size : (first + width) * size]

        key_high, key_low = split(columns(4))
        query_high, query_low = split(columns(3))
        four = jnp.concatenate([key_high, key_low, query_high, query_low], axis=0)
        strength, factor, overlap = columns(0), columns(1), columns(2)
        left = jnp.concatenate([key_high, key_low, key_high], axis=0)
        left = jnp.concatenate([left, jnp.zeros((size - 3 * count, size), left.dtype)], axis=0)
        left = left.astype(jnp.float32).T.astype(jnp.bfloat16)[:, 0 : 3 * count]
        wide = diagonal(four)
        fetch(step).wait()
        memory = held[rows].reshape(count * size, size).astype(jnp.bfloat16)
        both = jnp.dot(wide, memory, preferred_element_type=jnp.float32)
        recalled = both[0:count] + both[count : 2 * count]
        asked = both[2 * count : 3 * count] + both[3 * count : 4 * count]
        change = strength * (columns(5) - factor * recalled)
        readout[rows, :] = factor * asked + overlap * change
        change_high, change_low = split(change)
        right = diagonal(jnp.concatenate([change_high, change_high, change_low], axis=0))
        outer = jnp.dot(left, right, preferred_element_type=jnp.float32)
        for b in range(count):
            spot = step * count + b
            held[spot] = factor[b : b + 1, :] * held[spot] + outer[:, b * size : (b + 1) * size]
        store(step).start()
        return carry

    lax.fori_loop(0, steps, body, 0)
    read = readout[...]
    scaling = lax.rsqrt(jnp.sum(read * read, axis=1, keepdims=True) / size + EPS)
    gate = packed_ref[:, 6 * size :]
    gated_ref[...] = (
        read * gain_ref[...].astype(jnp.float32) * (gate / (1.0 + jnp.exp(-gate)))
    ).astype(jnp.bfloat16)
    tall = jnp.broadcast_to(scaling, (total, 128))
    if total < 128:
        tall = jnp.concatenate([tall, jnp.zeros((128 - total, 128), jnp.float32)], axis=0)
    flat_ref[...] = tall.T[0:SMALL, 0:total].astype(jnp.bfloat16)
    for step in range(steps):
        store(step).wait()


def state_step(state, packed, head_gain):
    count, size, _ = state.shape
    steps = count // min(16, count)
    anywhere = pl.BlockSpec(memory_space=pl.ANY)
    return pl.pallas_call(
        state_kernel,
        in_specs=[anywhere, VMEM, VMEM],
        out_specs=[anywhere, VMEM, VMEM],
        out_shape=[
            jax.ShapeDtypeStruct(state.shape, state.dtype),
            jax.ShapeDtypeStruct((count, size), jnp.bfloat16),
            jax.ShapeDtypeStruct((SMALL, count), jnp.bfloat16),
        ],
        scratch_shapes=[
            pltpu.VMEM(state.shape, state.dtype),
            pltpu.VMEM((count, size), jnp.float32),
            pltpu.SemaphoreType.DMA((steps,)),
            pltpu.SemaphoreType.DMA((steps,)),
        ],
    )(state, packed, head_gain.reshape(1, size))


def output_kernel(
    heads,
    groups,
    stream_ref,
    gated_ref,
    scaling_ref,
    weight_hbm,
    out_ref,
    weight_ref,
    weight_sem,
    all_gated,
    all_scaling,
    columns,
    held,
    core_out,
    core_in,
    hop_out,
    hop_in,
    gated_send,
    gated_recv,
    scaling_send,
    scaling_recv,
    core_send,
    core_recv,
    hop_send,
    hop_recv,
):
    me = lax.axis_index("tp")
    place = me % heads
    group = me // heads
    rows, cols = stream_ref.shape
    batch = all_gated.shape[0]
    group_rows = batch // groups
    dims = heads.bit_length() - 2
    chips = 1 << dims
    sibling = flip(me, (0,))
    neighbours = [flip(me, (bit,)) for bit in range(1, dims + 1)]
    others = [place + heads * ((group + j) % groups) for j in range(1, groups)]
    weight_copy = pltpu.make_async_copy(weight_hbm, weight_ref, weight_sem)
    weight_copy.start()
    enter([sibling] + neighbours + others)
    own_rows = pl.ds(pl.multiple_of(group * group_rows, group_rows), group_rows)
    copies = []
    arriving = []
    for j in range(1, groups):
        for source, target, send, recv in (
            (gated_ref, all_gated.at[own_rows], gated_send, gated_recv),
            (scaling_ref, all_scaling.at[group], scaling_send, scaling_recv),
        ):
            copy = remote(source, target, send.at[j - 1], recv.at[j - 1], others[j - 1])
            copy.start()
            copies.append(copy)
    all_gated[own_rows, :] = gated_ref[...]
    all_scaling[group] = scaling_ref[...]
    for copy in copies:
        copy.wait_recv()
    weight_copy.wait()
    wide = max(group_rows, 128)
    for g in range(groups):
        flat = all_scaling[g].astype(jnp.float32)
        if wide > group_rows:
            flat = jnp.concatenate(
                [flat, jnp.zeros((SMALL, wide - group_rows), jnp.float32)], axis=1
            )
        flat = jnp.concatenate([flat, jnp.zeros((128 - SMALL, wide), jnp.float32)], axis=0)
        columns[g * group_rows : (g + 1) * group_rows, :] = flat.T[0:group_rows]

    def relative(owner, mask):
        bits = tuple(bit for bit in range(1, dims + 1) if mask >> (bit - 1) & 1)
        begin = flip(owner, bits) * rows
        return pl.ds(pl.multiple_of(begin, rows), rows)

    def head_rows(owner, masks):
        picks = [relative(owner, mask) for mask in masks]
        left = jnp.concatenate([all_gated[pick, :] for pick in picks], axis=0)
        scale = jnp.concatenate([columns[pick, 0:1] for pick in picks], axis=0)
        product = lax.dot_general(
            left, weight_ref[...], (((1,), (1,)), ((), ())), preferred_element_type=jnp.float32
        )
        return product * scale

    core_copies = [
        remote(
            core_out.at[mask], core_in.at[mask], core_send.at[mask], core_recv.at[mask], sibling
        )
        for mask in range(chips)
    ]
    batch_of = min(4, chips)
    sweep = list(range(chips - 1, -1, -1))
    for first in range(0, chips, batch_of):
        masks = sweep[first : first + batch_of]
        product = head_rows(flip(place, (0,)), masks).astype(jnp.bfloat16)
        for i, mask in enumerate(masks):
            core_out[mask] = product[i * rows : (i + 1) * rows]
            core_copies[mask].start()
    for first in range(0, chips, batch_of):
        masks = sweep[first : first + batch_of]
        product = head_rows(place, masks)
        for i, mask in enumerate(masks):
            held[mask] = product[i * rows : (i + 1) * rows]

    parts = parts_of(cols, dims)
    hops = []
    waiting = [[] for _ in range(dims)]

    def cross(step, p, mask):
        (start, width), order = parts[p]
        if step == dims or not mask >> (order[step] - 1) & 1:
            return
        span = pl.ds(start, width)
        landed = mask - (1 << (order[step] - 1))
        hop_out[step, landed, :, span] = held[mask, :, span].astype(jnp.bfloat16)
        copy = remote(
            hop_out.at[step, landed, :, span],
            hop_in.at[step, landed, :, span],
            hop_send.at[step, p, landed],
            hop_recv.at[step, p, landed],
            neighbours[order[step] - 1],
        )
        copy.start()
        hops.append(copy)
        waiting[step].append((p, landed, span, copy))

    for mask in sweep:
        core_copies[mask].wait_recv()
        held[mask] += core_in[mask].astype(jnp.float32)
        for p in range(len(parts)):
            cross(0, p, mask)
    for step in range(dims):
        for p, landed, span, copy in waiting[step]:
            copy.wait_recv()
            held[landed, :, span] += hop_in[step, landed, :, span].astype(jnp.float32)
            cross(step + 1, p, landed)
    out_ref[...] = (stream_ref[...].astype(jnp.float32) + held[0]).astype(jnp.bfloat16)
    for copy in copies + core_copies + hops:
        copy.wait_send()


def output(stream, gated, scaling, out_weight, heads, groups):
    rows, cols = stream.shape
    batch = rows * heads
    group_rows, size = gated.shape
    dims = heads.bit_length() - 2
    chips = 1 << dims
    parts = len(parts_of(cols, dims))
    extra = groups - 1
    dma = pltpu.SemaphoreType.DMA
    anywhere = pl.BlockSpec(memory_space=pl.ANY)
    return pl.pallas_call(
        functools.partial(output_kernel, heads, groups),
        in_specs=[VMEM] * 3 + [anywhere],
        out_specs=VMEM,
        out_shape=jax.ShapeDtypeStruct(stream.shape, stream.dtype),
        scratch_shapes=[
            pltpu.VMEM(out_weight.shape, out_weight.dtype),
            dma(()),
            pltpu.VMEM((batch, size), jnp.bfloat16),
            pltpu.VMEM((groups, SMALL, group_rows), jnp.bfloat16),
            pltpu.VMEM((batch, 128), jnp.float32),
            pltpu.VMEM((chips, rows, cols), jnp.float32),
            pltpu.VMEM((chips, rows, cols), jnp.bfloat16),
            pltpu.VMEM((chips, rows, cols), jnp.bfloat16),
            pltpu.VMEM((dims, chips, rows, cols), jnp.bfloat16),
            pltpu.VMEM((dims, chips, rows, cols), jnp.bfloat16),
            dma((extra,)),
            dma((extra,)),
            dma((extra,)),
            dma((extra,)),
            dma((chips,)),
            dma((chips,)),
            dma((dims, parts, chips)),
            dma((dims, parts, chips)),
        ],
        compiler_params=pltpu.CompilerParams(
            collective_id=1, has_side_effects=True
        ),
    )(stream, gated, scaling, out_weight)


def masked(mask, dims):
    return tuple(bit for bit in range(1, dims + 1) if mask >> (bit - 1) & 1)


def fused_kernel(
    heads,
    groups,
    stream_ref,
    gain_ref,
    query_w,
    key_w,
    value_w,
    gate_w,
    write_w,
    decay_w,
    rate_ref,
    head_gain_ref,
    out_w,
    state_ref,
    held,
    packed,
    result,
    gathered,
    weights,
    side_w,
    gain_row,
    gains,
    both_w,
    partial,
    partial_side,
    sent,
    received,
    small_sent,
    small_received,
    work,
    gated,
    left,
    acc,
    hop_out,
    hop_in,
    last_out,
    last_in,
    up_out,
    up_in,
    local_sems,
    state_sems,
    pair_sems,
    ici_send,
    ici_recv,
    core_send,
    core_recv,
    main_send,
    main_recv,
    small_send,
    small_recv,
    gated_send,
    gated_recv,
    hop_send,
    hop_recv,
    last_send,
    last_recv,
    up_send,
    up_recv,
):
    me = lax.axis_index("tp")
    place = me % heads
    group = me // heads
    core = place % 2
    rows, cols = stream_ref.shape
    size = query_w.shape[1]
    dims = heads.bit_length() - 2
    chips = 1 << dims
    flats = chips // 2
    chip_rows = 2 * rows
    count = held.shape[0] // state_sems.shape[0]
    sibling = flip(me, (0,))
    neighbours = [flip(me, (bit,)) for bit in range(1, dims + 1)]
    partner = place + heads * ((group + 1) % groups)
    partner_sibling = flip(partner, (0,))
    own_cols = pl.ds(pl.multiple_of(group * cols, cols), cols)
    upper = place // flats // 2
    keep = (upper + group) % 2

    fetches = [
        pltpu.make_async_copy(
            weight, weights.at[:, i * size : (i + 1) * size], local_sems.at[i]
        )
        for i, weight in enumerate((query_w, key_w, value_w, gate_w))
    ] + [
        pltpu.make_async_copy(
            source.at[:, own_cols], side_w.at[i * heads : (i + 1) * heads], local_sems.at[4 + i]
        )
        for i, source in enumerate((write_w, decay_w))
    ]
    own_half = pltpu.make_async_copy(out_w, both_w.at[:, 0:size], local_sems.at[6])
    other_half = remote(
        out_w, both_w.at[:, size : 2 * size], pair_sems.at[0], pair_sems.at[1], sibling
    )

    def fetch(step):
        spot = pl.ds(pl.multiple_of(step * count, count), count)
        return pltpu.make_async_copy(state_ref.at[spot], held.at[spot], state_sems.at[step])

    for copy in fetches:
        copy.start()
    enter([sibling] + neighbours + [partner, partner_sibling])

    half = rows // 2
    top = dims
    parts = [(0, (top, 1, 2)), (half, (top, 2, 1))]

    def block(device_place, p):
        begin = device_place * rows + parts[p][0]
        return gathered.at[pl.ds(pl.multiple_of(begin, half), half), :]

    sends = []

    def pass_on(p, bits):
        order = parts[p][1]
        step = max([order.index(bit) for bit in bits], default=-1)
        target = block(flip(place, bits), p)
        source = target if bits else stream_ref.at[parts[p][0] : parts[p][0] + half, :]
        for later in range(step + 1, dims):
            landed = key_of(bits + (order[later],))
            copy = remote(
                source,
                target,
                ici_send.at[p, landed],
                ici_recv.at[p, landed],
                flip(me, (order[later],)),
            )
            copy.start()
            sends.append(copy)
        own = key_of(bits)
        copy = remote(source, target, core_send.at[p, own], core_recv.at[p, own], sibling)
        copy.start()
        sends.append(copy)

    def relay(p, mask):
        bits = masked(mask, dims)
        target = block(flip(place, bits), p)
        remote(target, target, ici_send.at[p, mask], ici_recv.at[p, mask], sibling).wait_recv()
        pass_on(p, bits)

    def from_sibling(mask):
        for p in range(2):
            target = block(flip(sibling % heads, masked(mask, dims)), p)
            remote(
                target, target, core_send.at[p, mask], core_recv.at[p, mask], sibling
            ).wait_recv()

    for p in range(2):
        pass_on(p, ())
    gathered[pl.ds(pl.multiple_of(place * rows, rows), rows), :] = stream_ref[...]
    gains[...] = gain_ref[...].astype(jnp.float32)
    tiles = cols // 128
    for i in range(tiles):
        gain_row[:, i * 128 : (i + 1) * 128] = gains[pl.ds(group * tiles + i, 1), :]
    for copy in fetches:
        copy.wait()
    for step in range(state_sems.shape[0]):
        fetch(step).start()
    own_half.start()

    main_copies = [
        remote(sent.at[c], received.at[c], main_send.at[c], main_recv.at[c], partner)
        for c in range(flats)
    ]
    small_copies = [
        remote(
            small_sent.at[c], small_received.at[c], small_send.at[c], small_recv.at[c], partner
        )
        for c in range(flats)
    ]

    def project(mask):
        c = mask % flats
        begin = flip(place, masked(mask, dims)) // 2 * chip_rows
        from_sibling(mask)
        x = gathered[pl.ds(pl.multiple_of(begin, chip_rows), chip_rows), :].astype(jnp.float32)
        gained = (x * gain_row[...]).astype(jnp.bfloat16)
        product = jnp.dot(gained, weights[...], preferred_element_type=jnp.float32)
        pre = lax.dot_general(
            gained, side_w[...], (((1,), (1,)), ((), ())), preferred_element_type=jnp.float32
        )
        spot = lax.broadcasted_iota(jnp.int32, pre.shape, 1)
        write = jnp.sum(jnp.where(spot == place, pre, 0.0), axis=1, keepdims=True)
        decay = jnp.sum(jnp.where(spot == place + heads, pre, 0.0), axis=1, keepdims=True)
        squares = jnp.sum(x * x, axis=1, keepdims=True)
        lane = lax.broadcasted_iota(jnp.int32, (chip_rows, 128), 1)
        side = jnp.where(
            lane == 0, write, jnp.where(lane == 1, decay, jnp.where(lane == 2, squares, 0.0))
        )
        away = (upper + mask // flats + group) % 2

        @pl.when(away == 1)
        def _():
            sent[c] = product.astype(jnp.bfloat16)
            main_copies[c].start()
            tall = jnp.concatenate(
                [side, jnp.zeros((128 - chip_rows, 128), jnp.float32)], axis=0
            ) if chip_rows < 128 else side
            small_sent[c] = tall.T[0:SMALL].astype(jnp.bfloat16)
            small_copies[c].start()

        @pl.when(away == 0)
        def _():
            partial[c] = product
            partial_side[c] = side

    spots = lax.broadcasted_iota(jnp.int32, (4 * count, size), 0) % count

    def diagonal(values):
        marks = spots[0 : values.shape[0]]
        return jnp.concatenate(
            [jnp.where(marks == b, values, jnp.zeros_like(values)) for b in range(count)], axis=1
        )

    def rounded(v):
        return v.astype(jnp.bfloat16).astype(jnp.float32)

    mine = lax.broadcasted_iota(jnp.int32, rate_ref.shape, 1) == place
    rate = jnp.sum(jnp.where(mine, rate_ref[...], 0.0), axis=1, keepdims=True)
    shares = []

    def recall(c):
        main_copies[c].wait_recv()
        small_copies[c].wait_recv()
        begin = flip(place, masked(c, dims)) // 2 % flats * chip_rows
        whole = pl.ds(pl.multiple_of(begin, chip_rows), chip_rows)
        total = partial[c] + received[c].astype(jnp.float32)
        flat = small_received[c].astype(jnp.float32)
        flat = jnp.concatenate([flat, jnp.zeros((128 - SMALL, flat.shape[1]), jnp.float32)], axis=0)
        side = partial_side[c] + flat.T[0:chip_rows]
        scale = lax.rsqrt(side[:, 2:3] / (cols * groups) + EPS)
        projected = rounded(total * scale)
        query = projected[:, :size]
        key = projected[:, size : 2 * size]
        query = query * lax.rsqrt(jnp.sum(query * query, axis=1, keepdims=True) + EPS) * size**-0.5
        key = key * lax.rsqrt(jnp.sum(key * key, axis=1, keepdims=True) + EPS)
        pre = rounded(side * scale)
        strength = jax.nn.sigmoid(pre[:, 0:1])
        decay = pre[:, 1:2]
        softplus = jnp.maximum(decay, 0.0) + jnp.log(1.0 + jnp.exp(-jnp.abs(decay)))
        factor = jnp.broadcast_to(jnp.exp(-rate * softplus), (chip_rows, size))
        overlap = jnp.sum(query * key, axis=1, keepdims=True)
        gate = projected[:, 3 * size :]
        lift = head_gain_ref[...].astype(jnp.float32) * (gate / (1.0 + jnp.exp(-gate)))
        packed[whole, 0:size] = key
        packed[whole, 2 * size : 3 * size] = factor
        work[:, 0:size] = query
        work[:, size : 2 * size] = projected[:, 2 * size : 3 * size]
        work[:, 2 * size : 3 * size] = lift
        work[:, 3 * size : 4 * size] = jnp.broadcast_to(strength, (chip_rows, size))
        work[:, 4 * size : 5 * size] = jnp.broadcast_to(overlap, (chip_rows, size))

        def body(i, carry):
            near = pl.ds(pl.multiple_of(i * count, count), count)
            step = begin // count + i
            spot = pl.ds(pl.multiple_of(begin + i * count, count), count)
            key_high, key_low = split(packed[spot, 0:size])
            query_high, query_low = split(work[near, 0:size])
            wide = diagonal(jnp.concatenate([key_high, key_low, query_high, query_low], axis=0))
            fetch(step).wait()
            memory = held[spot].reshape(count * size, size).astype(jnp.bfloat16)
            both = jnp.dot(wide, memory, preferred_element_type=jnp.float32)
            recalled = both[0:count] + both[count : 2 * count]
            asked = both[2 * count : 3 * count] + both[3 * count : 4 * count]
            factors = packed[spot, 2 * size : 3 * size]
            change = work[near, 3 * size : 4 * size] * (
                work[near, size : 2 * size] - factors * recalled
            )
            packed[spot, size : 2 * size] = change
            read = factors * asked + work[near, 4 * size : 5 * size] * change
            scaling = lax.rsqrt(jnp.sum(read * read, axis=1, keepdims=True) / size + EPS)
            gated[c, near, :] = (read * scaling * work[near, 2 * size : 3 * size]).astype(
                jnp.bfloat16
            )
            return carry

        lax.fori_loop(0, chip_rows // count, body, 0)
        span = pl.ds(c * rows, rows)
        same = gated.at[c, pl.ds(pl.multiple_of(core * rows, rows), rows), :]
        cross = gated.at[c, pl.ds(pl.multiple_of((1 - core) * rows, rows), rows), :]
        for i, (source, phase, j, device) in enumerate(
            (
                (same, 1, 0, partner),
                (cross, 1, 1, partner_sibling),
                (cross, 0, 1, sibling),
            )
        ):
            copy = remote(
                source,
                left.at[phase, span, j * size : (j + 1) * size],
                gated_send.at[c, i],
                gated_recv.at[c, i],
                device,
            )
            copy.start()
            shares.append(copy)
        left[0, c * rows : (c + 1) * rows, 0:size] = gated[
            c, pl.ds(pl.multiple_of(core * rows, rows), rows), :
        ]

    wide_half = cols // 2
    turns = [(1, 2), (2, 1)]
    hops = []

    def expand(phase):
        lefts = left[phase]
        for p, (first, second) in enumerate(turns):
            span = slice(p * wide_half, (p + 1) * wide_half)
            product = lax.dot_general(
                lefts,
                both_w[span, :],
                (((1,), (1,)), ((), ())),
                preferred_element_type=jnp.float32,
            )
            for i, c in enumerate((first + second, first)):
                hop_out[phase, p, i] = product[c * rows : (c + 1) * rows].astype(jnp.bfloat16)
                copy = hop(phase, p, i)
                copy.start()
                hops.append(copy)
            acc[phase, 0, :, span] = product[0:rows]
            acc[phase, 1, :, span] = product[second * rows : (second + 1) * rows]

    def hop(phase, p, i):
        return remote(
            hop_out.at[phase, p, i],
            hop_in.at[phase, p, i],
            hop_send.at[phase, p, i],
            hop_recv.at[phase, p, i],
            neighbours[turns[p][0] - 1],
        )

    def last(phase, p):
        return remote(
            last_out.at[phase, p],
            last_in.at[phase, p],
            last_send.at[phase, p],
            last_recv.at[phase, p],
            neighbours[turns[p][1] - 1],
        )

    def up(p):
        return remote(
            up_out.at[p], up_in.at[p], up_send.at[p], up_recv.at[p], neighbours[top - 1]
        )

    def second_hop(phase):
        for p in range(2):
            span = slice(p * wide_half, (p + 1) * wide_half)
            hop(phase, p, 0).wait_recv()
            last_out[phase, p] = (
                acc[phase, 1, :, span] + hop_in[phase, p, 0].astype(jnp.float32)
            ).astype(jnp.bfloat16)
            last(phase, p).start()
        for p in range(2):
            span = slice(p * wide_half, (p + 1) * wide_half)
            hop(phase, p, 1).wait_recv()
            acc[phase, 0, :, span] += hop_in[phase, p, 1].astype(jnp.float32)

    def settle(phase):
        for p in range(2):
            span = slice(p * wide_half, (p + 1) * wide_half)
            last(phase, p).wait_recv()
            total = acc[phase, 0, :, span] + last_in[phase, p].astype(jnp.float32)

            @pl.when(keep == phase)
            def _():
                acc[phase, 0, :, span] = total

            @pl.when(keep != phase)
            def _():
                up_out[p] = total.astype(jnp.bfloat16)
                up(p).start()

    x, y, z = 1, 2, flats
    project(0)
    other_half.start()
    relay(0, z)
    relay(0, x)
    relay(1, z)
    relay(1, y)
    relay(0, y)
    relay(1, x)
    project(z)
    relay(0, x + z)
    project(x)
    relay(1, y + z)
    relay(1, x + z)
    relay(0, y + z)
    project(y)
    relay(0, x + y)
    relay(1, x + y)
    project(x + z)
    project(y + z)
    project(x + y)
    recall(0)
    relay(0, x + y + z)
    relay(1, x + y + z)
    project(x + y + z)
    for c in range(1, flats):
        recall(c)
    own_half.wait()
    other_half.wait_recv()
    for c in range(flats):
        shares[3 * c + 2].wait_recv()
    expand(0)
    for c in range(flats):
        shares[3 * c].wait_recv()
        shares[3 * c + 1].wait_recv()
    expand(1)
    second_hop(0)
    second_hop(1)
    settle(0)
    settle(1)
    for p in range(2):
        span = slice(p * wide_half, (p + 1) * wide_half)
        up(p).wait_recv()
        result[:, span] = (
            stream_ref[:, span].astype(jnp.float32)
            + acc[keep, 0, :, span]
            + up_in[p].astype(jnp.float32)
        ).astype(jnp.bfloat16)
    for copy in sends + main_copies + small_copies + shares + hops + [other_half]:
        copy.wait_send()
    for p in range(2):
        up(p).wait_send()
        for phase in range(2):
            last(phase, p).wait_send()


def fused(stream, norm_gain, weights, write_weight, decay_weight, rate, head_gain, out_weight, state, groups):
    rows, cols = stream.shape
    heads = rate.shape[0]
    size = weights[0].shape[1]
    dims = heads.bit_length() - 2
    flats = (1 << dims) // 2
    group_rows = state.shape[0]
    steps = group_rows // min(16, group_rows)
    batch = rows * heads
    chip_rows = 2 * rows
    dma = pltpu.SemaphoreType.DMA
    anywhere = pl.BlockSpec(memory_space=pltpu.HBM)
    f32, bf16 = jnp.float32, jnp.bfloat16
    return pl.pallas_call(
        functools.partial(fused_kernel, heads, groups),
        in_specs=[VMEM] * 2 + [anywhere] * 6 + [VMEM] * 2 + [anywhere] * 2,
        out_specs=[VMEM] * 3,
        out_shape=[
            pltpu.VMEM(state.shape, state.dtype),
            pltpu.VMEM((group_rows, 3 * size), f32),
            pltpu.VMEM(stream.shape, stream.dtype),
        ],
        scratch_shapes=[
            pltpu.VMEM((batch, cols), bf16),
            pltpu.VMEM((cols, 4 * size), bf16),
            pltpu.VMEM((2 * heads, cols), bf16),
            pltpu.VMEM((1, cols), f32),
            pltpu.VMEM((groups * cols // 128, 128), f32),
            pltpu.VMEM((cols, 2 * size), bf16),
            pltpu.VMEM((flats, chip_rows, 4 * size), f32),
            pltpu.VMEM((flats, chip_rows, 128), f32),
            pltpu.VMEM((flats, chip_rows, 4 * size), bf16),
            pltpu.VMEM((flats, chip_rows, 4 * size), bf16),
            pltpu.VMEM((flats, SMALL, max(128, chip_rows)), bf16),
            pltpu.VMEM((flats, SMALL, max(128, chip_rows)), bf16),
            pltpu.VMEM((chip_rows, 5 * size), f32),
            pltpu.VMEM((flats, chip_rows, size), bf16),
            pltpu.VMEM((2, flats * rows, 2 * size), bf16),
            pltpu.VMEM((2, 2, rows, cols), f32),
            pltpu.VMEM((2, 2, 2, rows, cols // 2), bf16),
            pltpu.VMEM((2, 2, 2, rows, cols // 2), bf16),
            pltpu.VMEM((2, 2, rows, cols // 2), bf16),
            pltpu.VMEM((2, 2, rows, cols // 2), bf16),
            pltpu.VMEM((2, rows, cols // 2), bf16),
            pltpu.VMEM((2, rows, cols // 2), bf16),
            dma((7,)),
            dma((steps,)),
            dma((2,)),
            dma((2, 2 * flats)),
            dma((2, 2 * flats)),
            dma((2, 2 * flats)),
            dma((2, 2 * flats)),
            dma((flats,)),
            dma((flats,)),
            dma((flats,)),
            dma((flats,)),
            dma((flats, 3)),
            dma((flats, 3)),
            dma((2, 2, 2)),
            dma((2, 2, 2)),
            dma((2, 2)),
            dma((2, 2)),
            dma((2,)),
            dma((2,)),
        ],
        compiler_params=pltpu.CompilerParams(
            collective_id=2, has_side_effects=True, vmem_limit_bytes=43 << 20
        ),
    )(
        stream,
        norm_gain.reshape(groups * cols // 128, 128),
        *weights,
        write_weight.T,
        decay_weight.T,
        rate.reshape(1, heads),
        head_gain.reshape(1, size),
        out_weight,
        state,
    )


def store_kernel(held, packed, result, new_ref, out_ref, fresh, sems, out_sem):
    total, size, _ = held.shape
    steps = sems.shape[0]
    count = total // steps
    copy_out = pltpu.make_async_copy(result, out_ref, out_sem)
    copy_out.start()

    def store(step):
        spot = pl.ds(pl.multiple_of(step * count, count), count)
        return pltpu.make_async_copy(fresh.at[spot], new_ref.at[spot], sems.at[step])

    spots = lax.broadcasted_iota(jnp.int32, (3 * count, size), 0) % count

    def body(step, carry):
        spot = pl.ds(pl.multiple_of(step * count, count), count)
        key_high, key_low = split(packed[spot, 0:size])
        change_high, change_low = split(packed[spot, size : 2 * size])
        factor = packed[spot, 2 * size : 3 * size]
        keys = jnp.concatenate([key_high, key_low, key_high], axis=0)
        keys = jnp.concatenate([keys, jnp.zeros((size - 3 * count, size), keys.dtype)], axis=0)
        keys = keys.astype(jnp.float32).T.astype(jnp.bfloat16)[:, 0 : 3 * count]
        changes = jnp.concatenate([change_high, change_high, change_low], axis=0)
        wide = jnp.concatenate(
            [jnp.where(spots == b, changes, jnp.zeros_like(changes)) for b in range(count)], axis=1
        )
        outer = jnp.dot(keys, wide, preferred_element_type=jnp.float32)
        for b in range(count):
            fresh[step * count + b] = (
                factor[b : b + 1, :] * held[step * count + b]
                + outer[:, b * size : (b + 1) * size]
            )
        store(step).start()
        return carry

    lax.fori_loop(0, steps, body, 0)
    for step in range(steps):
        store(step).wait()
    copy_out.wait()


def store(held, packed, result):
    total = held.shape[0]
    steps = total // min(16, total)
    anywhere = pl.BlockSpec(memory_space=pl.ANY)
    return pl.pallas_call(
        store_kernel,
        in_specs=[VMEM] * 3,
        out_specs=[anywhere] * 2,
        out_shape=[
            jax.ShapeDtypeStruct(held.shape, held.dtype),
            jax.ShapeDtypeStruct(result.shape, result.dtype),
        ],
        scratch_shapes=[
            pltpu.VMEM(held.shape, held.dtype),
            pltpu.SemaphoreType.DMA((steps,)),
            pltpu.SemaphoreType.DMA(()),
        ],
        compiler_params=pltpu.CompilerParams(vmem_limit_bytes=20 << 20),
    )(held, packed, result)


def per_device(
    stream,
    norm_gain,
    query_weight,
    key_weight,
    value_weight,
    gate_weight,
    write_weight,
    decay_weight,
    decay_rate,
    head_gain,
    out_weight,
    state,
):
    heads = decay_rate.shape[0]
    groups = lax.axis_size("tp") // heads
    weights = (query_weight, key_weight, value_weight, gate_weight)
    rows, cols = stream.shape
    if groups == 2 and heads == 16 and rows % 32 == 0 and rows <= 64 and cols % 256 == 0:
        held, packed, result = fused(
            stream,
            norm_gain,
            weights,
            write_weight,
            decay_weight,
            decay_rate,
            head_gain,
            out_weight,
            state,
            groups,
        )
        updated, result = store(held, packed, result)
        return (result, updated)
    packed = project(
        stream, norm_gain, weights, write_weight, decay_weight, decay_rate, heads, groups
    )
    updated, gated, scaling = state_step(state, packed, head_gain)
    result = output(stream, gated, scaling, out_weight, heads, groups)
    return (result, updated)


def solution(mesh):
    placed = (
        P("tp", None),
        P(),
        P("tp", None),
        P("tp", None),
        P("tp", None),
        P("tp", None),
        P(),
        P(),
        P(),
        P(),
        P("tp", None),
        P("tp", None, None),
    )
    return jax.shard_map(
        per_device,
        mesh=mesh,
        in_specs=placed,
        out_specs=(P("tp", None), P("tp", None, None)),
        check_vma=False,
    )
```

```python
import functools

import jax
import jax.numpy as jnp
from jax import lax
from jax.experimental import pallas as pl
from jax.experimental.pallas import tpu as pltpu
from jax.sharding import PartitionSpec as P

EPS = 1e-06
MESH = pl.DeviceIdType.MESH
VMEM = pl.BlockSpec(memory_space=pltpu.VMEM)
SMALL = 16


def flip(me, bits):
    other = me
    for bit in bits:
        other = other + (1 - 2 * ((me // (1 << bit)) % 2)) * (1 << bit)
    return other


def parts_of(cols, dims):
    tiles = cols // 128
    count = max(1, min(dims, tiles))
    cuts = [tiles * i // count * 128 for i in range(count + 1)]
    ranges = [(cuts[i], cuts[i + 1] - cuts[i]) for i in range(count)]
    orders = [[1 + (i + j) % dims for j in range(dims)] for i in range(count)]
    return list(zip(ranges, orders))


def masks_of(order):
    sets = [((), -1)]
    for step in range(len(order)):
        sets = sets + [(bits + (order[step],), step) for bits, _ in sets]
    return sets


def key_of(bits):
    return sum(1 << (bit - 1) for bit in bits)


def enter(devices):
    barrier = pltpu.get_barrier_semaphore()
    for device in devices:
        pl.semaphore_signal(barrier, inc=1, device_id=(device,), device_id_type=MESH)
    pl.semaphore_wait(barrier, len(devices))


def remote(source, target, send_sem, recv_sem, device):
    return pltpu.make_async_remote_copy(
        src_ref=source,
        dst_ref=target,
        send_sem=send_sem,
        recv_sem=recv_sem,
        device_id=(device,),
        device_id_type=MESH,
    )


def project_kernel(
    heads,
    groups,
    stream_ref,
    gain_ref,
    query_w,
    key_w,
    value_w,
    gate_w,
    write_w,
    decay_w,
    rate_ref,
    packed_out,
    gathered,
    weights,
    write_t,
    decay_t,
    gains,
    local_sems,
    partial,
    sent,
    received,
    small_sent,
    small_received,
    turned,
    ici_send,
    ici_recv,
    core_send,
    core_recv,
    group_send,
    group_recv,
    small_send,
    small_recv,
):
    me = lax.axis_index("tp")
    place = me % heads
    group = me // heads
    rows, cols = stream_ref.shape
    batch = gathered.shape[0]
    group_rows = batch // groups
    dims = heads.bit_length() - 2
    sibling = flip(me, (0,))
    neighbours = [flip(me, (bit,)) for bit in range(1, dims + 1)]
    others = [place + heads * ((group + j) % groups) for j in range(1, groups)]
    size = query_w.shape[1]
    own_cols = pl.ds(pl.multiple_of(group * cols, cols), cols)
    fetches = [
        pltpu.make_async_copy(
            weight, weights.at[:, i * size : (i + 1) * size], local_sems.at[i]
        )
        for i, weight in enumerate((query_w, key_w, value_w, gate_w))
    ] + [
        pltpu.make_async_copy(source.at[:, own_cols], target, local_sems.at[4 + i])
        for i, (source, target) in enumerate(((write_w, write_t), (decay_w, decay_t)))
    ]
    for fetch in fetches:
        fetch.start()
    enter([sibling] + neighbours + others)

    halves = 2 if rows % 32 == 0 and group_rows % rows == 0 else 1
    part_rows = rows // halves
    half_batch = batch // halves
    ranges = parts_of(cols, dims)

    def half_rows(h, device_place):
        begin = h * half_batch + device_place * part_rows
        return pl.ds(pl.multiple_of(begin, part_rows), part_rows)

    def block(h, device_place, part):
        return gathered.at[half_rows(h, device_place), pl.ds(part[0][0], part[0][1])]

    sends = []
    core_copies = [[] for _ in range(halves)]

    def pass_on(h, p, part, bits, step):
        order = part[1]
        origin = flip(place, bits)
        target = block(h, origin, part)
        if bits:
            source = target
        else:
            source = stream_ref.at[
                pl.ds(h * part_rows, part_rows), pl.ds(part[0][0], part[0][1])
            ]
        for later in range(step + 1, dims):
            landed = key_of(bits + (order[later],))
            copy = remote(
                source,
                target,
                ici_send.at[h, p, landed],
                ici_recv.at[h, p, landed],
                flip(me, (order[later],)),
            )
            copy.start()
            sends.append(copy)
        own = key_of(bits)
        copy = remote(source, target, core_send.at[h, p, own], core_recv.at[h, p, own], sibling)
        copy.start()
        core_copies[h].append(copy)

    def begin(h):
        for p, part in enumerate(ranges):
            pass_on(h, p, part, (), -1)

    def relay(h, index):
        for p, part in enumerate(ranges):
            bits, step = masks_of(part[1])[index]
            landed = key_of(bits)
            target = block(h, flip(place, bits), part)
            remote(
                target, target, ici_send.at[h, p, landed], ici_recv.at[h, p, landed], sibling
            ).wait_recv()
            pass_on(h, p, part, bits, step)

    early = max(2, 1 << (dims - 1))
    begin(0)
    for h in range(halves):
        gathered[half_rows(h, place), :] = stream_ref[h * part_rows : (h + 1) * part_rows, :]
    relay(0, 1)
    for h in range(1, halves):
        begin(h)
    for index in range(2, 1 << dims):
        relay(0, index)
    for h in range(1, halves):
        for index in range(1, early):
            relay(h, index)
    for copy in core_copies[0]:
        copy.wait_recv()

    gains[...] = gain_ref[...].astype(jnp.float32)
    gain = jnp.concatenate(
        [gains[pl.ds(group * (cols // 128) + i, 1), :] for i in range(cols // 128)], axis=1
    )
    for fetch in fetches:
        fetch.wait()

    def project(begin, count, at):
        x = gathered[pl.ds(begin, count), :].astype(jnp.float32)
        gained = (x * gain).astype(jnp.bfloat16)
        partial[pl.ds(at, count), :] = jnp.dot(
            gained, weights[...], preferred_element_type=jnp.float32
        )
        mine = lax.broadcasted_iota(jnp.int32, (count, heads), 1) == place
        pre = [
            jnp.sum(
                jnp.where(
                    mine,
                    lax.dot_general(
                        gained,
                        w[...],
                        (((1,), (1,)), ((), ())),
                        preferred_element_type=jnp.float32,
                    ),
                    0.0,
                ),
                axis=1,
                keepdims=True,
            )
            for w in (write_t, decay_t)
        ]
        squares = jnp.sum(x * x, axis=1, keepdims=True)
        lane = lax.broadcasted_iota(jnp.int32, (count, 128), 1)
        return jnp.where(
            lane == 0, pre[0], jnp.where(lane == 1, pre[1], jnp.where(lane == 2, squares, 0.0))
        )

    copies = []
    wide = max(group_rows, 128)
    count = group_rows // halves

    def half_of(h, target_group):
        begin = h * half_batch + target_group * count
        return pl.multiple_of(begin, count)

    for h in range(halves):
        if h:
            for index in range(early, 1 << dims):
                relay(h, index)
            for copy in core_copies[h]:
                copy.wait_recv()
        for j in range(1, groups):
            spot = slice(h * count, (h + 1) * count)
            side = project(half_of(h, (group + j) % groups), count, 0)
            sent[j - 1, spot] = partial[0:count].astype(jnp.bfloat16)
            turned[spot] = side
            routes = [(sent.at[j - 1, spot], received.at[j - 1, spot], group_send, group_recv)]
            flat = turned[...].T
            small_sent[j - 1, :, spot] = flat[0:SMALL, spot].astype(jnp.bfloat16)
            routes.append(
                (
                    small_sent.at[j - 1, :, spot],
                    small_received.at[j - 1, :, spot],
                    small_send,
                    small_recv,
                )
            )
            for source, target, send, recv in routes:
                copy = remote(
                    source, target, send.at[h, j - 1], recv.at[h, j - 1], others[j - 1]
                )
                copy.start()
                copies.append(copy)
    for h in range(halves):
        turned[h * count : (h + 1) * count] = project(half_of(h, group), count, h * count)
    total = partial[...]
    flat = turned[...].T[0:SMALL, :]
    for copy in copies:
        copy.wait_recv()
    for j in range(1, groups):
        total = total + received[j - 1].astype(jnp.float32)
    small_total = flat[:, 0:group_rows]
    for j in range(1, groups):
        small_total = small_total + small_received[j - 1].astype(jnp.float32)
    turned_back = jnp.concatenate(
        [small_total, jnp.zeros((SMALL, wide - group_rows), jnp.float32)], axis=1
    ) if wide > group_rows else small_total
    side = jnp.concatenate(
        [turned_back, jnp.zeros((128 - SMALL, wide), jnp.float32)], axis=0
    ).T[0:group_rows]
    scale = lax.rsqrt(side[:, 2:3] / (cols * groups) + EPS)

    def rounded(v):
        return v.astype(jnp.bfloat16).astype(jnp.float32)

    projected = rounded(total * scale)
    query = projected[:, :size]
    key = projected[:, size : 2 * size]
    query = query * lax.rsqrt(jnp.sum(query * query, axis=1, keepdims=True) + EPS) * size**-0.5
    key = key * lax.rsqrt(jnp.sum(key * key, axis=1, keepdims=True) + EPS)
    pre = rounded(side * scale)
    strength = jax.nn.sigmoid(pre[:, 0:1])
    mine = lax.broadcasted_iota(jnp.int32, rate_ref.shape, 1) == place
    rate = jnp.sum(jnp.where(mine, rate_ref[...], 0.0), axis=1, keepdims=True)
    decay = pre[:, 1:2]
    softplus = jnp.maximum(decay, 0.0) + jnp.log(1.0 + jnp.exp(-jnp.abs(decay)))
    factor = jnp.exp(-rate * softplus)
    overlap = jnp.sum(query * key, axis=1, keepdims=True)
    results = [jnp.broadcast_to(v, (group_rows, size)) for v in (strength, factor, overlap)]
    results += [query, key, projected[:, 2 * size :]]
    for i, v in enumerate(results):
        span = pl.ds(i * size, v.shape[1])
        if halves == 1:
            packed_out[:, span] = v
            continue
        for h in range(halves):
            for q in range(group_rows // rows):
                to, come = q * rows + h * part_rows, h * count + q * part_rows
                packed_out[to : to + part_rows, span] = v[come : come + part_rows]
    for copy in sends + sum(core_copies, []) + copies:
        copy.wait_send()


def project(stream, norm_gain, weights, write_weight, decay_weight, rate, heads, groups):
    rows, cols = stream.shape
    batch = rows * heads
    group_rows = batch // groups
    size = weights[0].shape[1]
    dims = heads.bit_length() - 2
    parts = len(parts_of(cols, dims))
    extra = groups - 1
    halves = 2
    dma = pltpu.SemaphoreType.DMA
    anywhere = pl.BlockSpec(memory_space=pl.ANY)
    return pl.pallas_call(
        functools.partial(project_kernel, heads, groups),
        in_specs=[VMEM] * 2 + [anywhere] * 6 + [VMEM],
        out_specs=VMEM,
        out_shape=jax.ShapeDtypeStruct((group_rows, 7 * size), jnp.float32),
        scratch_shapes=[
            pltpu.VMEM((batch, cols), jnp.bfloat16),
            pltpu.VMEM((cols, 4 * size), jnp.bfloat16),
            pltpu.VMEM((heads, cols), jnp.bfloat16),
            pltpu.VMEM((heads, cols), jnp.bfloat16),
            pltpu.VMEM((groups * cols // 128, 128), jnp.float32),
            dma((6,)),
            pltpu.VMEM((group_rows, 4 * size), jnp.float32),
            pltpu.VMEM((extra, group_rows, 4 * size), jnp.bfloat16),
            pltpu.VMEM((extra, group_rows, 4 * size), jnp.bfloat16),
            pltpu.VMEM((extra, SMALL, group_rows), jnp.bfloat16),
            pltpu.VMEM((extra, SMALL, group_rows), jnp.bfloat16),
            pltpu.VMEM((max(group_rows, 128), 128), jnp.float32),
            dma((halves, parts, 1 << dims)),
            dma((halves, parts, 1 << dims)),
            dma((halves, parts, 1 << dims)),
            dma((halves, parts, 1 << dims)),
            dma((halves, extra)),
            dma((halves, extra)),
            dma((halves, extra)),
            dma((halves, extra)),
        ],
        compiler_params=pltpu.CompilerParams(
            collective_id=0, has_side_effects=True
        ),
    )(
        stream,
        norm_gain.reshape(groups * cols // 128, 128),
        *weights,
        write_weight.T,
        decay_weight.T,
        rate.reshape(1, heads),
    )


def split(v):
    high = v.astype(jnp.bfloat16)
    return high, (v - high.astype(jnp.float32)).astype(jnp.bfloat16)


def state_kernel(
    state_ref, packed_ref, gain_ref, new_ref, gated_ref, flat_ref, held, readout, in_sems, out_sems
):
    total, size, _ = state_ref.shape
    steps = in_sems.shape[0]
    count = total // steps

    def rows_of(step):
        return pl.ds(pl.multiple_of(step * count, count), count)

    def fetch(step):
        rows = rows_of(step)
        return pltpu.make_async_copy(state_ref.at[rows], held.at[rows], in_sems.at[step])

    def store(step):
        rows = rows_of(step)
        return pltpu.make_async_copy(held.at[rows], new_ref.at[rows], out_sems.at[step])

    for step in range(steps):
        fetch(step).start()
    spots = lax.broadcasted_iota(jnp.int32, (4 * count, size), 0) % count

    def diagonal(rows):
        marks = spots[0 : rows.shape[0]]
        return jnp.concatenate(
            [jnp.where(marks == b, rows, jnp.zeros_like(rows)) for b in range(count)], axis=1
        )

    def body(step, carry):
        rows = rows_of(step)

        def columns(first, width=1):
            return packed_ref[rows, first * size : (first + width) * size]

        key_high, key_low = split(columns(4))
        query_high, query_low = split(columns(3))
        four = jnp.concatenate([key_high, key_low, query_high, query_low], axis=0)
        strength, factor, overlap = columns(0), columns(1), columns(2)
        left = jnp.concatenate([key_high, key_low, key_high], axis=0)
        left = jnp.concatenate([left, jnp.zeros((size - 3 * count, size), left.dtype)], axis=0)
        left = left.astype(jnp.float32).T.astype(jnp.bfloat16)[:, 0 : 3 * count]
        wide = diagonal(four)
        fetch(step).wait()
        memory = held[rows].reshape(count * size, size).astype(jnp.bfloat16)
        both = jnp.dot(wide, memory, preferred_element_type=jnp.float32)
        recalled = both[0:count] + both[count : 2 * count]
        asked = both[2 * count : 3 * count] + both[3 * count : 4 * count]
        change = strength * (columns(5) - factor * recalled)
        readout[rows, :] = factor * asked + overlap * change
        change_high, change_low = split(change)
        right = diagonal(jnp.concatenate([change_high, change_high, change_low], axis=0))
        outer = jnp.dot(left, right, preferred_element_type=jnp.float32)
        for b in range(count):
            spot = step * count + b
            held[spot] = factor[b : b + 1, :] * held[spot] + outer[:, b * size : (b + 1) * size]
        store(step).start()
        return carry

    lax.fori_loop(0, steps, body, 0)
    read = readout[...]
    scaling = lax.rsqrt(jnp.sum(read * read, axis=1, keepdims=True) / size + EPS)
    gate = packed_ref[:, 6 * size :]
    gated_ref[...] = (
        read * gain_ref[...].astype(jnp.float32) * (gate / (1.0 + jnp.exp(-gate)))
    ).astype(jnp.bfloat16)
    tall = jnp.broadcast_to(scaling, (total, 128))
    if total < 128:
        tall = jnp.concatenate([tall, jnp.zeros((128 - total, 128), jnp.float32)], axis=0)
    flat_ref[...] = tall.T[0:SMALL, 0:total].astype(jnp.bfloat16)
    for step in range(steps):
        store(step).wait()


def state_step(state, packed, head_gain):
    count, size, _ = state.shape
    steps = count // min(16, count)
    anywhere = pl.BlockSpec(memory_space=pl.ANY)
    return pl.pallas_call(
        state_kernel,
        in_specs=[anywhere, VMEM, VMEM],
        out_specs=[anywhere, VMEM, VMEM],
        out_shape=[
            jax.ShapeDtypeStruct(state.shape, state.dtype),
            jax.ShapeDtypeStruct((count, size), jnp.bfloat16),
            jax.ShapeDtypeStruct((SMALL, count), jnp.bfloat16),
        ],
        scratch_shapes=[
            pltpu.VMEM(state.shape, state.dtype),
            pltpu.VMEM((count, size), jnp.float32),
            pltpu.SemaphoreType.DMA((steps,)),
            pltpu.SemaphoreType.DMA((steps,)),
        ],
    )(state, packed, head_gain.reshape(1, size))


def output_kernel(
    heads,
    groups,
    stream_ref,
    gated_ref,
    scaling_ref,
    weight_hbm,
    out_ref,
    weight_ref,
    weight_sem,
    all_gated,
    all_scaling,
    columns,
    held,
    core_out,
    core_in,
    hop_out,
    hop_in,
    gated_send,
    gated_recv,
    scaling_send,
    scaling_recv,
    core_send,
    core_recv,
    hop_send,
    hop_recv,
):
    me = lax.axis_index("tp")
    place = me % heads
    group = me // heads
    rows, cols = stream_ref.shape
    batch = all_gated.shape[0]
    group_rows = batch // groups
    dims = heads.bit_length() - 2
    chips = 1 << dims
    sibling = flip(me, (0,))
    neighbours = [flip(me, (bit,)) for bit in range(1, dims + 1)]
    others = [place + heads * ((group + j) % groups) for j in range(1, groups)]
    weight_copy = pltpu.make_async_copy(weight_hbm, weight_ref, weight_sem)
    weight_copy.start()
    enter([sibling] + neighbours + others)
    own_rows = pl.ds(pl.multiple_of(group * group_rows, group_rows), group_rows)
    copies = []
    arriving = []
    for j in range(1, groups):
        for source, target, send, recv in (
            (gated_ref, all_gated.at[own_rows], gated_send, gated_recv),
            (scaling_ref, all_scaling.at[group], scaling_send, scaling_recv),
        ):
            copy = remote(source, target, send.at[j - 1], recv.at[j - 1], others[j - 1])
            copy.start()
            copies.append(copy)
    all_gated[own_rows, :] = gated_ref[...]
    all_scaling[group] = scaling_ref[...]
    for copy in copies:
        copy.wait_recv()
    weight_copy.wait()
    wide = max(group_rows, 128)
    for g in range(groups):
        flat = all_scaling[g].astype(jnp.float32)
        if wide > group_rows:
            flat = jnp.concatenate(
                [flat, jnp.zeros((SMALL, wide - group_rows), jnp.float32)], axis=1
            )
        flat = jnp.concatenate([flat, jnp.zeros((128 - SMALL, wide), jnp.float32)], axis=0)
        columns[g * group_rows : (g + 1) * group_rows, :] = flat.T[0:group_rows]

    def relative(owner, mask):
        bits = tuple(bit for bit in range(1, dims + 1) if mask >> (bit - 1) & 1)
        begin = flip(owner, bits) * rows
        return pl.ds(pl.multiple_of(begin, rows), rows)

    def head_rows(owner, masks):
        picks = [relative(owner, mask) for mask in masks]
        left = jnp.concatenate([all_gated[pick, :] for pick in picks], axis=0)
        scale = jnp.concatenate([columns[pick, 0:1] for pick in picks], axis=0)
        product = lax.dot_general(
            left, weight_ref[...], (((1,), (1,)), ((), ())), preferred_element_type=jnp.float32
        )
        return product * scale

    core_copies = [
        remote(
            core_out.at[mask], core_in.at[mask], core_send.at[mask], core_recv.at[mask], sibling
        )
        for mask in range(chips)
    ]
    batch_of = min(4, chips)
    sweep = list(range(chips - 1, -1, -1))
    for first in range(0, chips, batch_of):
        masks = sweep[first : first + batch_of]
        product = head_rows(flip(place, (0,)), masks).astype(jnp.bfloat16)
        for i, mask in enumerate(masks):
            core_out[mask] = product[i * rows : (i + 1) * rows]
            core_copies[mask].start()
    for first in range(0, chips, batch_of):
        masks = sweep[first : first + batch_of]
        product = head_rows(place, masks)
        for i, mask in enumerate(masks):
            held[mask] = product[i * rows : (i + 1) * rows]

    parts = parts_of(cols, dims)
    hops = []
    waiting = [[] for _ in range(dims)]

    def cross(step, p, mask):
        (start, width), order = parts[p]
        if step == dims or not mask >> (order[step] - 1) & 1:
            return
        span = pl.ds(start, width)
        landed = mask - (1 << (order[step] - 1))
        hop_out[step, landed, :, span] = held[mask, :, span].astype(jnp.bfloat16)
        copy = remote(
            hop_out.at[step, landed, :, span],
            hop_in.at[step, landed, :, span],
            hop_send.at[step, p, landed],
            hop_recv.at[step, p, landed],
            neighbours[order[step] - 1],
        )
        copy.start()
        hops.append(copy)
        waiting[step].append((p, landed, span, copy))

    for mask in sweep:
        core_copies[mask].wait_recv()
        held[mask] += core_in[mask].astype(jnp.float32)
        for p in range(len(parts)):
            cross(0, p, mask)
    for step in range(dims):
        for p, landed, span, copy in waiting[step]:
            copy.wait_recv()
            held[landed, :, span] += hop_in[step, landed, :, span].astype(jnp.float32)
            cross(step + 1, p, landed)
    out_ref[...] = (stream_ref[...].astype(jnp.float32) + held[0]).astype(jnp.bfloat16)
    for copy in copies + core_copies + hops:
        copy.wait_send()


def output(stream, gated, scaling, out_weight, heads, groups):
    rows, cols = stream.shape
    batch = rows * heads
    group_rows, size = gated.shape
    dims = heads.bit_length() - 2
    chips = 1 << dims
    parts = len(parts_of(cols, dims))
    extra = groups - 1
    dma = pltpu.SemaphoreType.DMA
    anywhere = pl.BlockSpec(memory_space=pl.ANY)
    return pl.pallas_call(
        functools.partial(output_kernel, heads, groups),
        in_specs=[VMEM] * 3 + [anywhere],
        out_specs=VMEM,
        out_shape=jax.ShapeDtypeStruct(stream.shape, stream.dtype),
        scratch_shapes=[
            pltpu.VMEM(out_weight.shape, out_weight.dtype),
            dma(()),
            pltpu.VMEM((batch, size), jnp.bfloat16),
            pltpu.VMEM((groups, SMALL, group_rows), jnp.bfloat16),
            pltpu.VMEM((batch, 128), jnp.float32),
            pltpu.VMEM((chips, rows, cols), jnp.float32),
            pltpu.VMEM((chips, rows, cols), jnp.bfloat16),
            pltpu.VMEM((chips, rows, cols), jnp.bfloat16),
            pltpu.VMEM((dims, chips, rows, cols), jnp.bfloat16),
            pltpu.VMEM((dims, chips, rows, cols), jnp.bfloat16),
            dma((extra,)),
            dma((extra,)),
            dma((extra,)),
            dma((extra,)),
            dma((chips,)),
            dma((chips,)),
            dma((dims, parts, chips)),
            dma((dims, parts, chips)),
        ],
        compiler_params=pltpu.CompilerParams(
            collective_id=1, has_side_effects=True
        ),
    )(stream, gated, scaling, out_weight)


def masked(mask, dims):
    return tuple(bit for bit in range(1, dims + 1) if mask >> (bit - 1) & 1)


def fused_kernel(
    heads,
    groups,
    stream_hbm,
    gain_hbm,
    query_w,
    key_w,
    value_w,
    gate_w,
    write_w,
    decay_w,
    rate_hbm,
    head_gain_hbm,
    out_w,
    state_ref,
    held,
    mine_out,
    rise_out,
    stream_ref,
    gain_ref,
    rate_ref,
    head_gain_ref,
    gathered,
    weights,
    side_w,
    gain_row,
    gains,
    four_w,
    partial,
    partial_side,
    sent,
    received,
    small_sent,
    small_received,
    packed,
    answers,
    gated,
    left,
    acc,
    hop_out,
    hop_in,
    local_sems,
    state_sems,
    pair_sems,
    send_sems,
    ici_recv,
    core_recv,
    main_recv,
    small_recv,
    gated_recv,
    hop_recv,
):
    me = lax.axis_index("tp")
    place = me % heads
    group = me // heads
    core = place % 2
    rows, cols = stream_ref.shape
    size = query_w.shape[1]
    dims = heads.bit_length() - 2
    chips = 1 << dims
    flats = chips // 2
    chip_rows = 2 * rows
    group_rows = flats * chip_rows
    count = 16
    x, y, z = 1, 2, flats
    sibling = flip(me, (0,))
    neighbours = [flip(me, (bit,)) for bit in range(1, dims + 1)]
    partner = place + heads * ((group + 1) % groups)
    peers = [sibling] + neighbours + [partner, flip(partner, (0,))]
    for h in range(2):
        there = flip(partner, (h + 1,))
        peers += [flip(neighbours[h], (0,)), there, flip(there, (0,))]
    own_cols = pl.ds(pl.multiple_of(group * cols, cols), cols)
    upper = place // flats // 2
    keep = (upper + group) % 2
    outer = 1 - keep

    barrier = pltpu.get_barrier_semaphore()
    for device in peers:
        pl.semaphore_signal(barrier, inc=1, device_id=(device,), device_id_type=MESH)
    early = [
        pltpu.make_async_copy(source, target, local_sems.at[i])
        for i, (source, target) in enumerate(
            (
                (stream_hbm, stream_ref),
                (gain_hbm, gain_ref),
                (rate_hbm, rate_ref),
                (head_gain_hbm, head_gain_ref),
            )
        )
    ]
    for copy in early:
        copy.start()
    for i, weight in enumerate((query_w, key_w, value_w, gate_w)):
        pltpu.make_async_copy(
            weight, weights.at[:, i * size : (i + 1) * size], local_sems.at[4]
        ).start()
    for i, source in enumerate((write_w, decay_w)):
        pltpu.make_async_copy(
            source.at[:, own_cols], side_w.at[i * heads : (i + 1) * heads], local_sems.at[5]
        ).start()
    weights_done = pltpu.make_async_copy(weights, weights, local_sems.at[4])
    side_done = pltpu.make_async_copy(side_w, side_w, local_sems.at[5])
    own_w = pltpu.make_async_copy(out_w, four_w.at[:, 0:size], local_sems.at[6])
    sibling_w = remote(
        out_w, four_w.at[:, size : 2 * size], pair_sems.at[0], pair_sems.at[1], sibling
    )
    pieces = 4
    wide_half = cols // 2
    tall = wide_half // pieces

    def beside_w(h, i, n=1):
        spot = slice(h * wide_half + i * tall, h * wide_half + (i + n) * tall)
        return remote(
            out_w.at[spot, :],
            four_w.at[spot, 2 * size : 3 * size],
            pair_sems.at[3],
            pair_sems.at[4 + h],
            neighbours[h],
        )

    def passed_w(h, n=1):
        spot = slice(h * wide_half, (h + n) * wide_half)
        return remote(
            four_w.at[spot, 2 * size : 3 * size],
            four_w.at[spot, 3 * size : 4 * size],
            pair_sems.at[2],
            pair_sems.at[6],
            sibling,
        )

    def fetch(c):
        spot = pl.ds(pl.multiple_of(c * chip_rows, chip_rows), chip_rows)
        return pltpu.make_async_copy(state_ref.at[spot], held.at[spot], state_sems.at[c])

    half = rows // 2
    top = dims
    parts = [(0, (top, 1, 2)), (half, (top, 2, 1))]

    def block(device_place, p, q):
        begin = device_place * rows + parts[p][0]
        return gathered.at[
            pl.ds(pl.multiple_of(begin, half), half), q * wide_half : (q + 1) * wide_half
        ]

    def pass_on(p, q, bits):
        order = parts[p][1]
        step = max([order.index(bit) for bit in bits], default=-1)
        target = block(flip(place, bits), p, q)
        source = target
        if not bits:
            source = stream_ref.at[
                parts[p][0] : parts[p][0] + half, q * wide_half : (q + 1) * wide_half
            ]
        for later in range(step + 1, dims):
            remote(
                source,
                target,
                send_sems.at[0],
                ici_recv.at[p, q, key_of(bits + (order[later],)) - 1],
                flip(me, (order[later],)),
            ).start()
        remote(source, target, send_sems.at[1], core_recv.at[key_of(bits)], sibling).start()

    def relay(p, q, mask):
        bits = masked(mask, dims)
        target = block(flip(place, bits), p, q)
        remote(target, target, send_sems.at[0], ici_recv.at[p, q, mask - 1], sibling).wait_recv()
        pass_on(p, q, bits)

    spot_x, spot_y = place // 2 % 2, place // 4 % 2

    def chip_of(c):
        return (spot_x + c) % 2 + 2 * ((spot_y + c // 2) % 2)

    def from_sibling(c, raised):
        level = (upper + raised) % 2
        begin = (level * flats + chip_of(c)) * chip_rows + (1 - core) * rows
        target = gathered.at[pl.ds(pl.multiple_of(begin, rows), rows), :]
        remote(
            target, target, send_sems.at[1], core_recv.at[c + flats * raised], sibling
        ).wait_recv()

    for copy in early:
        copy.wait()
    pl.semaphore_wait(barrier, len(peers))
    for q in range(2):
        for p in range(2):
            pass_on(p, q, ())
    sibling_w.start()
    gathered[pl.ds(pl.multiple_of(place * rows, rows), rows), :] = stream_ref[...]
    gains[...] = gain_ref[...].astype(jnp.float32)
    tiles = cols // 128
    for i in range(tiles):
        gain_row[:, i * 128 : (i + 1) * 128] = gains[pl.ds(group * tiles + i, 1), :]
    weights_done.wait()
    side_done.wait()
    for c in range(flats):
        fetch(chip_of(c)).start()
    own_w.start()

    def project(begin, high):
        x = gathered[pl.ds(pl.multiple_of(begin, chip_rows), high), :].astype(jnp.float32)
        gained = (x * gain_row[...]).astype(jnp.bfloat16)
        product = jnp.dot(gained, weights[...], preferred_element_type=jnp.float32)
        pre = lax.dot_general(
            gained, side_w[...], (((1,), (1,)), ((), ())), preferred_element_type=jnp.float32
        )
        spot = lax.broadcasted_iota(jnp.int32, pre.shape, 1)
        write = jnp.sum(jnp.where(spot == place, pre, 0.0), axis=1, keepdims=True)
        decay = jnp.sum(jnp.where(spot == place + heads, pre, 0.0), axis=1, keepdims=True)
        squares = jnp.sum(x * x, axis=1, keepdims=True)
        lane = lax.broadcasted_iota(jnp.int32, (high, 128), 1)
        side = jnp.where(
            lane == 0, write, jnp.where(lane == 1, decay, jnp.where(lane == 2, squares, 0.0))
        )
        return product, side

    away_begin = (group + 1) % groups * group_rows

    def main_copy(c):
        return remote(sent.at[c], received.at[c], send_sems.at[2], main_recv.at[c], partner)

    def small_copy(c):
        return remote(
            small_sent.at[c], small_received.at[c], send_sems.at[3], small_recv.at[c], partner
        )

    def project_away(c, raised):
        from_sibling(c, raised)
        product, side = project(away_begin + chip_of(c) * chip_rows, chip_rows)
        sent[c] = product.astype(jnp.bfloat16)
        main_copy(c).start()
        if chip_rows < 128:
            side = jnp.concatenate(
                [side, jnp.zeros((128 - chip_rows, 128), jnp.float32)], axis=0
            )
        small_sent[c] = side.T[0:SMALL].astype(jnp.bfloat16)
        small_copy(c).start()

    def project_here(j, raised):
        for c in range(2 * j, 2 * j + 2):
            from_sibling(c, raised)
        pair = (spot_y + j) % 2
        spot = pl.ds(pl.multiple_of(pair * 2 * chip_rows, 2 * chip_rows), 2 * chip_rows)
        product, side = project(group * group_rows + pair * 2 * chip_rows, 2 * chip_rows)
        partial[spot, :] = product
        partial_side[spot, :] = side

    def marks(n):
        return lax.broadcasted_iota(jnp.int32, (n * count, size), 0) % count

    def diagonal(values, spots):
        return jnp.concatenate(
            [jnp.where(spots == b, values, jnp.zeros_like(values)) for b in range(count)], axis=1
        )

    def rounded(v):
        return v.astype(jnp.bfloat16).astype(jnp.float32)

    mine = lax.broadcasted_iota(jnp.int32, rate_ref.shape, 1) == place
    rate = jnp.sum(jnp.where(mine, rate_ref[...], 0.0), axis=1, keepdims=True)

    def recall(c):
        main_copy(c).wait_recv()
        small_copy(c).wait_recv()
        begin = chip_of(c) * chip_rows
        whole = pl.ds(pl.multiple_of(begin, chip_rows), chip_rows)
        total = partial[whole, :] + received[c].astype(jnp.float32)
        flat = small_received[c].astype(jnp.float32)
        flat = jnp.concatenate([flat, jnp.zeros((128 - SMALL, flat.shape[1]), jnp.float32)], axis=0)
        side = partial_side[whole, :] + flat.T[0:chip_rows]
        scale = lax.rsqrt(side[:, 2:3] / (cols * groups) + EPS)
        projected = rounded(total * scale)
        query = projected[:, :size]
        key = projected[:, size : 2 * size]
        query = query * lax.rsqrt(jnp.sum(query * query, axis=1, keepdims=True) + EPS) * size**-0.5
        key = key * lax.rsqrt(jnp.sum(key * key, axis=1, keepdims=True) + EPS)
        key_high, key_low = split(key)
        query_high, query_low = split(query)
        fetch(chip_of(c)).wait()
        spots = marks(4)
        for i in range(chip_rows // count):
            near = slice(i * count, (i + 1) * count)
            spot = pl.ds(pl.multiple_of(begin + i * count, count), count)
            four = [v[near] for v in (key_high, key_low, query_high, query_low)]
            wide = diagonal(jnp.concatenate(four, axis=0), spots)
            memory = held[spot].reshape(count * size, size).astype(jnp.bfloat16)
            both = jnp.dot(wide, memory, preferred_element_type=jnp.float32)
            answers[0, near, :] = both[0:count] + both[count : 2 * count]
            answers[1, near, :] = both[2 * count : 3 * count] + both[3 * count : 4 * count]
        pre = rounded(side * scale)
        strength = jax.nn.sigmoid(pre[:, 0:1])
        decay = pre[:, 1:2]
        softplus = jnp.maximum(decay, 0.0) + jnp.log(1.0 + jnp.exp(-jnp.abs(decay)))
        factor = jnp.broadcast_to(jnp.exp(-rate * softplus), (chip_rows, size))
        overlap = jnp.sum(query * key, axis=1, keepdims=True)
        gate = projected[:, 3 * size :]
        lift = head_gain_ref[...].astype(jnp.float32) * (gate / (1.0 + jnp.exp(-gate)))
        change = strength * (projected[:, 2 * size : 3 * size] - factor * answers[0])
        read = factor * answers[1] + overlap * change
        scaling = lax.rsqrt(jnp.sum(read * read, axis=1, keepdims=True) / size + EPS)
        gated[c] = (read * scaling * lift).astype(jnp.bfloat16)
        same = gated.at[c, pl.ds(pl.multiple_of(core * rows, rows), rows), :]
        cross = gated.at[c, pl.ds(pl.multiple_of((1 - core) * rows, rows), rows), :]
        for h in range(2 if c else 1):
            gap, row = (c // 2, c % 2) if h else (c % 2, c // 2)
            span = slice(row * rows, (row + 1) * rows)
            first = 2 * gap
            there = flip(partner, (h + 1,)) if gap else partner
            here = neighbours[h] if gap else me
            for source, phase, j, device in (
                (same, 1, first, there),
                (cross, 1, first + 1, flip(there, (0,))),
                (cross, 0, first + 1, flip(here, (0,))),
                (same, 0, first, here),
            ):
                target = left.at[h, phase, span, j * size : (j + 1) * size]
                if phase or j:
                    remote(source, target, send_sems.at[4], gated_recv.at[h, phase], device).start()
                else:
                    left[h, 0, span, 0:size] = gated[
                        c, pl.ds(pl.multiple_of(core * rows, rows), rows), :
                    ]
        packed[c, 0] = key
        packed[c, 1] = change
        packed[c, 2] = factor

    def update(c):
        begin = chip_of(c) * chip_rows
        spots = marks(3)

        def body(i, carry):
            near = pl.ds(pl.multiple_of(i * count, count), count)
            key_high, key_low = split(packed[c, 0, near, :])
            change_high, change_low = split(packed[c, 1, near, :])
            factor = packed[c, 2, near, :]
            keys = jnp.concatenate([key_high, key_low, key_high], axis=0)
            keys = jnp.concatenate([keys, jnp.zeros((size - 3 * count, size), keys.dtype)], axis=0)
            keys = keys.astype(jnp.float32).T.astype(jnp.bfloat16)[:, 0 : 3 * count]
            wide = diagonal(jnp.concatenate([change_high, change_high, change_low], axis=0), spots)
            outer_product = jnp.dot(keys, wide, preferred_element_type=jnp.float32)
            for b in range(count):
                spot = begin + i * count + b
                held[spot] = (
                    factor[b : b + 1, :] * held[spot]
                    + outer_product[:, b * size : (b + 1) * size]
                )
            return carry

        lax.fori_loop(0, chip_rows // count, body, 0)

    def hop(phase, h):
        return remote(
            hop_out.at[phase, h],
            hop_in.at[phase, h],
            send_sems.at[5],
            hop_recv.at[phase, h],
            neighbours[1 - h],
        )

    def expand(phase):
        for h in range(2):
            span = slice(h * wide_half, (h + 1) * wide_half)
            lefts = left[h, phase]
            if h:
                upper_rows = jnp.concatenate(
                    [left[0, phase, 0:rows, 0 : 2 * size], lefts[0:rows, 2 * size :]], axis=1
                )
                lefts = jnp.concatenate([upper_rows, lefts[rows:]], axis=0)
            product = lax.dot_general(
                lefts,
                four_w[span, :],
                (((1,), (1,)), ((), ())),
                preferred_element_type=jnp.float32,
            )
            hop_out[phase, h] = product[rows:].astype(jnp.bfloat16)
            hop(phase, h).start()
            acc[phase, :, span] = product[0:rows]

    def settle(phase):
        for q in range(2):
            span = slice(q * wide_half, (q + 1) * wide_half)
            hop(phase, q).wait_recv()
            total = acc[phase, :, span] + hop_in[phase, q].astype(jnp.float32)

            @pl.when(keep == phase)
            def _():
                mine_out[:, span] = total

            @pl.when(keep != phase)
            def _():
                rise_out[:, span] = total.astype(jnp.bfloat16)

    def gated_bytes(h, phase):
        blocks = (6, 8) if h == 0 else (5, 6)
        return gathered.at[0:rows, 0 : blocks[phase] * size]

    def whole_left(phase):
        for h in range(2):
            target = gated_bytes(h, phase)
            remote(target, target, send_sems.at[4], gated_recv.at[h, phase], sibling).wait_recv()

    def relays(masks):
        for q in range(2):
            for p, mask in masks:
                relay(p, q, mask)

    def send_beside(first, last):
        for i in range(first, last):
            for h in range(2):
                beside_w(h, i).start()

    def pass_weights(h):
        beside_w(h, 0, pieces).wait_recv()
        passed_w(h).start()

    def weights_ready():
        own_w.wait()
        sibling_w.wait_recv()
        passed_w(0, 2).wait_recv()

    def drain():
        sibling_w.wait_send()
        passed_w(0, 2).wait_send()
        for h in range(2):
            beside_w(h, 0, pieces).wait_send()
        ici_rows = rows * (chips - 1)
        for i, ref in enumerate(
            (gathered.at[0:ici_rows, :], gathered.at[0 : rows * chips, :], sent, small_sent)
        ):
            remote(ref, ref, send_sems.at[i], main_recv.at[0], partner).wait_send()
        for phase in range(2):
            for h in range(2):
                target = gated_bytes(h, phase)
                remote(target, target, send_sems.at[4], gated_recv.at[0, 0], sibling).wait_send()
        remote(hop_out, hop_in, send_sems.at[5], hop_recv.at[0, 0], sibling).wait_send()

    @pl.when(outer == 1)
    def _():
        relays([(0, z), (1, z)])
        project_away(0, 1)
        relays([(0, x), (1, y), (1, x), (0, y)])
        send_beside(0, 1)
        relays([(0, x + z), (1, y + z), (1, x + z), (0, y + z)])
        project_away(1, 1)
        project_away(2, 1)
        send_beside(1, pieces)
        project_here(0, 0)
        relays([(0, x + y + z), (1, x + y + z)])
        project_away(3, 1)
        relays([(0, x + y), (1, x + y)])
        project_here(1, 0)

    @pl.when(outer == 0)
    def _():
        project_away(0, 0)
        relays([(0, x), (1, y), (1, x), (0, y)])
        project_away(1, 0)
        project_away(2, 0)
        relays([(0, z), (1, z)])
        relays([(0, x + y), (1, x + y)])
        project_away(3, 0)
        relays([(0, x + z), (1, y + z), (1, x + z), (0, y + z)])
        send_beside(0, pieces)
        project_here(0, 1)
        relays([(0, x + y + z), (1, x + y + z)])
        project_here(1, 1)

    recall(0)
    recall(1)
    recall(2)
    recall(3)
    pass_weights(0)
    pass_weights(1)
    weights_ready()
    whole_left(0)
    expand(0)
    update(0)
    update(1)
    whole_left(1)
    expand(1)
    update(2)
    settle(0)
    update(3)
    settle(1)
    drain()


def fused(
    stream,
    norm_gain,
    weights,
    write_weight,
    decay_weight,
    rate,
    head_gain,
    out_weight,
    state,
    groups,
):
    rows, cols = stream.shape
    heads = rate.shape[0]
    size = weights[0].shape[1]
    chips = heads // 2
    flats = chips // 2
    batch = rows * heads
    chip_rows = 2 * rows
    dma = pltpu.SemaphoreType.DMA
    anywhere = pl.BlockSpec(memory_space=pltpu.HBM)
    f32, bf16 = jnp.float32, jnp.bfloat16
    return pl.pallas_call(
        functools.partial(fused_kernel, heads, groups),
        in_specs=[anywhere] * 12,
        out_specs=[VMEM] * 3,
        out_shape=[
            pltpu.VMEM(state.shape, state.dtype),
            pltpu.VMEM(stream.shape, f32),
            pltpu.VMEM(stream.shape, bf16),
        ],
        scratch_shapes=[
            pltpu.VMEM(stream.shape, stream.dtype),
            pltpu.VMEM((groups * cols // 128, 128), bf16),
            pltpu.VMEM((1, heads), f32),
            pltpu.VMEM((1, size), bf16),
            pltpu.VMEM((batch, cols), bf16),
            pltpu.VMEM((cols, 4 * size), bf16),
            pltpu.VMEM((2 * heads, cols), bf16),
            pltpu.VMEM((1, cols), f32),
            pltpu.VMEM((groups * cols // 128, 128), f32),
            pltpu.VMEM((cols, 4 * size), bf16),
            pltpu.VMEM((flats * chip_rows, 4 * size), f32),
            pltpu.VMEM((flats * chip_rows, 128), f32),
            pltpu.VMEM((flats, chip_rows, 4 * size), bf16),
            pltpu.VMEM((flats, chip_rows, 4 * size), bf16),
            pltpu.VMEM((flats, SMALL, max(128, chip_rows)), bf16),
            pltpu.VMEM((flats, SMALL, max(128, chip_rows)), bf16),
            pltpu.VMEM((flats, 3, chip_rows, size), f32),
            pltpu.VMEM((2, chip_rows, size), f32),
            pltpu.VMEM((flats, chip_rows, size), bf16),
            pltpu.VMEM((2, 2, 2 * rows, 4 * size), bf16),
            pltpu.VMEM((2, rows, cols), f32),
            pltpu.VMEM((2, 2, rows, cols // 2), bf16),
            pltpu.VMEM((2, 2, rows, cols // 2), bf16),
            dma((7,)),
            dma((flats,)),
            dma((7,)),
            dma((6,)),
            dma((2, 2, chips - 1)),
            dma((chips,)),
            dma((flats,)),
            dma((flats,)),
            dma((2, 2)),
            dma((2, 2)),
        ],
        compiler_params=pltpu.CompilerParams(
            collective_id=2, has_side_effects=True, vmem_limit_bytes=43 << 20
        ),
    )(
        stream,
        norm_gain.reshape(groups * cols // 128, 128),
        *weights,
        write_weight.T,
        decay_weight.T,
        rate.reshape(1, heads),
        head_gain.reshape(1, size),
        out_weight,
        state,
    )


def store_kernel(held, new_ref, sems):
    steps = sems.shape[0]
    count = held.shape[0] // steps
    copies = []
    for step in range(steps):
        spot = slice(step * count, (step + 1) * count)
        copies.append(pltpu.make_async_copy(held.at[spot], new_ref.at[spot], sems.at[step]))
        copies[-1].start()
    for copy in copies:
        copy.wait()


def store(held):
    steps = min(8, held.shape[0])
    return pl.pallas_call(
        store_kernel,
        in_specs=[VMEM],
        out_specs=pl.BlockSpec(memory_space=pl.ANY),
        out_shape=jax.ShapeDtypeStruct(held.shape, held.dtype),
        scratch_shapes=[pltpu.SemaphoreType.DMA((steps,))],
        cost_estimate=pl.CostEstimate(
            flops=1000 * held.size, bytes_accessed=4 * held.size, transcendentals=0
        ),
        compiler_params=pltpu.CompilerParams(vmem_limit_bytes=4 << 20),
    )(held)


def per_device(
    stream,
    norm_gain,
    query_weight,
    key_weight,
    value_weight,
    gate_weight,
    write_weight,
    decay_weight,
    decay_rate,
    head_gain,
    out_weight,
    state,
):
    heads = decay_rate.shape[0]
    groups = lax.axis_size("tp") // heads
    weights = (query_weight, key_weight, value_weight, gate_weight)
    rows, cols = stream.shape
    if groups == 2 and heads == 16 and rows % 32 == 0 and rows <= 64 and cols % 256 == 0:
        held, mine, rise = fused(
            stream,
            norm_gain,
            weights,
            write_weight,
            decay_weight,
            decay_rate,
            head_gain,
            out_weight,
            state,
            groups,
        )
        span = heads // 2
        pairs = [
            (i, i + span * (1 - 2 * (i // span % 2))) for i in range(lax.axis_size("tp"))
        ]
        arrived = lax.ppermute(rise, "tp", pairs)
        updated = store(held)
        result = stream.astype(jnp.float32) + mine + arrived.astype(jnp.float32)
        return (result.astype(stream.dtype), updated)
    packed = project(
        stream, norm_gain, weights, write_weight, decay_weight, decay_rate, heads, groups
    )
    updated, gated, scaling = state_step(state, packed, head_gain)
    result = output(stream, gated, scaling, out_weight, heads, groups)
    return (result, updated)


def solution(mesh):
    placed = (
        P("tp", None),
        P(),
        P("tp", None),
        P("tp", None),
        P("tp", None),
        P("tp", None),
        P(),
        P(),
        P(),
        P(),
        P("tp", None),
        P("tp", None, None),
    )
    return jax.shard_map(
        per_device,
        mesh=mesh,
        in_specs=placed,
        out_specs=(P("tp", None), P("tp", None, None)),
        check_vma=False,
    )
```

```python
import functools

import jax
import jax.numpy as jnp
from jax import lax
from jax.experimental import pallas as pl
from jax.experimental.pallas import tpu as pltpu
from jax.sharding import PartitionSpec as P

EPS = 1e-06
MESH = pl.DeviceIdType.MESH
VMEM = pl.BlockSpec(memory_space=pltpu.VMEM)
SMALL = 16
TINY = 8


def flip(me, bits):
    other = me
    for bit in bits:
        other = other + (1 - 2 * ((me // (1 << bit)) % 2)) * (1 << bit)
    return other


def parts_of(cols, dims):
    tiles = cols // 128
    count = max(1, min(dims, tiles))
    cuts = [tiles * i // count * 128 for i in range(count + 1)]
    ranges = [(cuts[i], cuts[i + 1] - cuts[i]) for i in range(count)]
    orders = [[1 + (i + j) % dims for j in range(dims)] for i in range(count)]
    return list(zip(ranges, orders))


def masks_of(order):
    sets = [((), -1)]
    for step in range(len(order)):
        sets = sets + [(bits + (order[step],), step) for bits, _ in sets]
    return sets


def key_of(bits):
    return sum(1 << (bit - 1) for bit in bits)


def enter(devices):
    barrier = pltpu.get_barrier_semaphore()
    for device in devices:
        pl.semaphore_signal(barrier, inc=1, device_id=(device,), device_id_type=MESH)
    pl.semaphore_wait(barrier, len(devices))


def remote(source, target, send_sem, recv_sem, device):
    return pltpu.make_async_remote_copy(
        src_ref=source,
        dst_ref=target,
        send_sem=send_sem,
        recv_sem=recv_sem,
        device_id=(device,),
        device_id_type=MESH,
    )


def project_kernel(
    heads,
    groups,
    stream_ref,
    gain_ref,
    query_w,
    key_w,
    value_w,
    gate_w,
    write_w,
    decay_w,
    rate_ref,
    packed_out,
    gathered,
    weights,
    write_t,
    decay_t,
    gains,
    local_sems,
    partial,
    sent,
    received,
    small_sent,
    small_received,
    turned,
    ici_send,
    ici_recv,
    core_send,
    core_recv,
    group_send,
    group_recv,
    small_send,
    small_recv,
):
    me = lax.axis_index("tp")
    place = me % heads
    group = me // heads
    rows, cols = stream_ref.shape
    batch = gathered.shape[0]
    group_rows = batch // groups
    dims = heads.bit_length() - 2
    sibling = flip(me, (0,))
    neighbours = [flip(me, (bit,)) for bit in range(1, dims + 1)]
    others = [place + heads * ((group + j) % groups) for j in range(1, groups)]
    size = query_w.shape[1]
    own_cols = pl.ds(pl.multiple_of(group * cols, cols), cols)
    fetches = [
        pltpu.make_async_copy(
            weight, weights.at[:, i * size : (i + 1) * size], local_sems.at[i]
        )
        for i, weight in enumerate((query_w, key_w, value_w, gate_w))
    ] + [
        pltpu.make_async_copy(source.at[:, own_cols], target, local_sems.at[4 + i])
        for i, (source, target) in enumerate(((write_w, write_t), (decay_w, decay_t)))
    ]
    for fetch in fetches:
        fetch.start()
    enter([sibling] + neighbours + others)

    halves = 2 if rows % 32 == 0 and group_rows % rows == 0 else 1
    part_rows = rows // halves
    half_batch = batch // halves
    ranges = parts_of(cols, dims)

    def half_rows(h, device_place):
        begin = h * half_batch + device_place * part_rows
        return pl.ds(pl.multiple_of(begin, part_rows), part_rows)

    def block(h, device_place, part):
        return gathered.at[half_rows(h, device_place), pl.ds(part[0][0], part[0][1])]

    sends = []
    core_copies = [[] for _ in range(halves)]

    def pass_on(h, p, part, bits, step):
        order = part[1]
        origin = flip(place, bits)
        target = block(h, origin, part)
        if bits:
            source = target
        else:
            source = stream_ref.at[
                pl.ds(h * part_rows, part_rows), pl.ds(part[0][0], part[0][1])
            ]
        for later in range(step + 1, dims):
            landed = key_of(bits + (order[later],))
            copy = remote(
                source,
                target,
                ici_send.at[h, p, landed],
                ici_recv.at[h, p, landed],
                flip(me, (order[later],)),
            )
            copy.start()
            sends.append(copy)
        own = key_of(bits)
        copy = remote(source, target, core_send.at[h, p, own], core_recv.at[h, p, own], sibling)
        copy.start()
        core_copies[h].append(copy)

    def begin(h):
        for p, part in enumerate(ranges):
            pass_on(h, p, part, (), -1)

    def relay(h, index):
        for p, part in enumerate(ranges):
            bits, step = masks_of(part[1])[index]
            landed = key_of(bits)
            target = block(h, flip(place, bits), part)
            remote(
                target, target, ici_send.at[h, p, landed], ici_recv.at[h, p, landed], sibling
            ).wait_recv()
            pass_on(h, p, part, bits, step)

    early = max(2, 1 << (dims - 1))
    begin(0)
    for h in range(halves):
        gathered[half_rows(h, place), :] = stream_ref[h * part_rows : (h + 1) * part_rows, :]
    relay(0, 1)
    for h in range(1, halves):
        begin(h)
    for index in range(2, 1 << dims):
        relay(0, index)
    for h in range(1, halves):
        for index in range(1, early):
            relay(h, index)
    for copy in core_copies[0]:
        copy.wait_recv()

    gains[...] = gain_ref[...].astype(jnp.float32)
    gain = jnp.concatenate(
        [gains[pl.ds(group * (cols // 128) + i, 1), :] for i in range(cols // 128)], axis=1
    )
    for fetch in fetches:
        fetch.wait()

    def project(begin, count, at):
        x = gathered[pl.ds(begin, count), :].astype(jnp.float32)
        gained = (x * gain).astype(jnp.bfloat16)
        partial[pl.ds(at, count), :] = jnp.dot(
            gained, weights[...], preferred_element_type=jnp.float32
        )
        mine = lax.broadcasted_iota(jnp.int32, (count, heads), 1) == place
        pre = [
            jnp.sum(
                jnp.where(
                    mine,
                    lax.dot_general(
                        gained,
                        w[...],
                        (((1,), (1,)), ((), ())),
                        preferred_element_type=jnp.float32,
                    ),
                    0.0,
                ),
                axis=1,
                keepdims=True,
            )
            for w in (write_t, decay_t)
        ]
        squares = jnp.sum(x * x, axis=1, keepdims=True)
        lane = lax.broadcasted_iota(jnp.int32, (count, 128), 1)
        return jnp.where(
            lane == 0, pre[0], jnp.where(lane == 1, pre[1], jnp.where(lane == 2, squares, 0.0))
        )

    copies = []
    wide = max(group_rows, 128)
    count = group_rows // halves

    def half_of(h, target_group):
        begin = h * half_batch + target_group * count
        return pl.multiple_of(begin, count)

    for h in range(halves):
        if h:
            for index in range(early, 1 << dims):
                relay(h, index)
            for copy in core_copies[h]:
                copy.wait_recv()
        for j in range(1, groups):
            spot = slice(h * count, (h + 1) * count)
            side = project(half_of(h, (group + j) % groups), count, 0)
            sent[j - 1, spot] = partial[0:count].astype(jnp.bfloat16)
            turned[spot] = side
            routes = [(sent.at[j - 1, spot], received.at[j - 1, spot], group_send, group_recv)]
            flat = turned[...].T
            small_sent[j - 1, :, spot] = flat[0:SMALL, spot].astype(jnp.bfloat16)
            routes.append(
                (
                    small_sent.at[j - 1, :, spot],
                    small_received.at[j - 1, :, spot],
                    small_send,
                    small_recv,
                )
            )
            for source, target, send, recv in routes:
                copy = remote(
                    source, target, send.at[h, j - 1], recv.at[h, j - 1], others[j - 1]
                )
                copy.start()
                copies.append(copy)
    for h in range(halves):
        turned[h * count : (h + 1) * count] = project(half_of(h, group), count, h * count)
    total = partial[...]
    flat = turned[...].T[0:SMALL, :]
    for copy in copies:
        copy.wait_recv()
    for j in range(1, groups):
        total = total + received[j - 1].astype(jnp.float32)
    small_total = flat[:, 0:group_rows]
    for j in range(1, groups):
        small_total = small_total + small_received[j - 1].astype(jnp.float32)
    turned_back = jnp.concatenate(
        [small_total, jnp.zeros((SMALL, wide - group_rows), jnp.float32)], axis=1
    ) if wide > group_rows else small_total
    side = jnp.concatenate(
        [turned_back, jnp.zeros((128 - SMALL, wide), jnp.float32)], axis=0
    ).T[0:group_rows]
    scale = lax.rsqrt(side[:, 2:3] / (cols * groups) + EPS)

    def rounded(v):
        return v.astype(jnp.bfloat16).astype(jnp.float32)

    projected = rounded(total * scale)
    query = projected[:, :size]
    key = projected[:, size : 2 * size]
    query = query * lax.rsqrt(jnp.sum(query * query, axis=1, keepdims=True) + EPS) * size**-0.5
    key = key * lax.rsqrt(jnp.sum(key * key, axis=1, keepdims=True) + EPS)
    pre = rounded(side * scale)
    strength = jax.nn.sigmoid(pre[:, 0:1])
    mine = lax.broadcasted_iota(jnp.int32, rate_ref.shape, 1) == place
    rate = jnp.sum(jnp.where(mine, rate_ref[...], 0.0), axis=1, keepdims=True)
    decay = pre[:, 1:2]
    softplus = jnp.maximum(decay, 0.0) + jnp.log(1.0 + jnp.exp(-jnp.abs(decay)))
    factor = jnp.exp(-rate * softplus)
    overlap = jnp.sum(query * key, axis=1, keepdims=True)
    results = [jnp.broadcast_to(v, (group_rows, size)) for v in (strength, factor, overlap)]
    results += [query, key, projected[:, 2 * size :]]
    for i, v in enumerate(results):
        span = pl.ds(i * size, v.shape[1])
        if halves == 1:
            packed_out[:, span] = v
            continue
        for h in range(halves):
            for q in range(group_rows // rows):
                to, come = q * rows + h * part_rows, h * count + q * part_rows
                packed_out[to : to + part_rows, span] = v[come : come + part_rows]
    for copy in sends + sum(core_copies, []) + copies:
        copy.wait_send()


def project(stream, norm_gain, weights, write_weight, decay_weight, rate, heads, groups):
    rows, cols = stream.shape
    batch = rows * heads
    group_rows = batch // groups
    size = weights[0].shape[1]
    dims = heads.bit_length() - 2
    parts = len(parts_of(cols, dims))
    extra = groups - 1
    halves = 2
    dma = pltpu.SemaphoreType.DMA
    anywhere = pl.BlockSpec(memory_space=pl.ANY)
    return pl.pallas_call(
        functools.partial(project_kernel, heads, groups),
        in_specs=[VMEM] * 2 + [anywhere] * 6 + [VMEM],
        out_specs=VMEM,
        out_shape=jax.ShapeDtypeStruct((group_rows, 7 * size), jnp.float32),
        scratch_shapes=[
            pltpu.VMEM((batch, cols), jnp.bfloat16),
            pltpu.VMEM((cols, 4 * size), jnp.bfloat16),
            pltpu.VMEM((heads, cols), jnp.bfloat16),
            pltpu.VMEM((heads, cols), jnp.bfloat16),
            pltpu.VMEM((groups * cols // 128, 128), jnp.float32),
            dma((6,)),
            pltpu.VMEM((group_rows, 4 * size), jnp.float32),
            pltpu.VMEM((extra, group_rows, 4 * size), jnp.bfloat16),
            pltpu.VMEM((extra, group_rows, 4 * size), jnp.bfloat16),
            pltpu.VMEM((extra, SMALL, group_rows), jnp.bfloat16),
            pltpu.VMEM((extra, SMALL, group_rows), jnp.bfloat16),
            pltpu.VMEM((max(group_rows, 128), 128), jnp.float32),
            dma((halves, parts, 1 << dims)),
            dma((halves, parts, 1 << dims)),
            dma((halves, parts, 1 << dims)),
            dma((halves, parts, 1 << dims)),
            dma((halves, extra)),
            dma((halves, extra)),
            dma((halves, extra)),
            dma((halves, extra)),
        ],
        compiler_params=pltpu.CompilerParams(
            collective_id=0, has_side_effects=True
        ),
    )(
        stream,
        norm_gain.reshape(groups * cols // 128, 128),
        *weights,
        write_weight.T,
        decay_weight.T,
        rate.reshape(1, heads),
    )


def split(v):
    high = v.astype(jnp.bfloat16)
    return high, (v - high.astype(jnp.float32)).astype(jnp.bfloat16)


def state_kernel(
    state_ref, packed_ref, gain_ref, new_ref, gated_ref, flat_ref, held, readout, in_sems, out_sems
):
    total, size, _ = state_ref.shape
    steps = in_sems.shape[0]
    count = total // steps

    def rows_of(step):
        return pl.ds(pl.multiple_of(step * count, count), count)

    def fetch(step):
        rows = rows_of(step)
        return pltpu.make_async_copy(state_ref.at[rows], held.at[rows], in_sems.at[step])

    def store(step):
        rows = rows_of(step)
        return pltpu.make_async_copy(held.at[rows], new_ref.at[rows], out_sems.at[step])

    for step in range(steps):
        fetch(step).start()
    spots = lax.broadcasted_iota(jnp.int32, (4 * count, size), 0) % count

    def diagonal(rows):
        marks = spots[0 : rows.shape[0]]
        return jnp.concatenate(
            [jnp.where(marks == b, rows, jnp.zeros_like(rows)) for b in range(count)], axis=1
        )

    def body(step, carry):
        rows = rows_of(step)

        def columns(first, width=1):
            return packed_ref[rows, first * size : (first + width) * size]

        key_high, key_low = split(columns(4))
        query_high, query_low = split(columns(3))
        four = jnp.concatenate([key_high, key_low, query_high, query_low], axis=0)
        strength, factor, overlap = columns(0), columns(1), columns(2)
        left = jnp.concatenate([key_high, key_low, key_high], axis=0)
        left = jnp.concatenate([left, jnp.zeros((size - 3 * count, size), left.dtype)], axis=0)
        left = left.astype(jnp.float32).T.astype(jnp.bfloat16)[:, 0 : 3 * count]
        wide = diagonal(four)
        fetch(step).wait()
        memory = held[rows].reshape(count * size, size).astype(jnp.bfloat16)
        both = jnp.dot(wide, memory, preferred_element_type=jnp.float32)
        recalled = both[0:count] + both[count : 2 * count]
        asked = both[2 * count : 3 * count] + both[3 * count : 4 * count]
        change = strength * (columns(5) - factor * recalled)
        readout[rows, :] = factor * asked + overlap * change
        change_high, change_low = split(change)
        right = diagonal(jnp.concatenate([change_high, change_high, change_low], axis=0))
        outer = jnp.dot(left, right, preferred_element_type=jnp.float32)
        for b in range(count):
            spot = step * count + b
            held[spot] = factor[b : b + 1, :] * held[spot] + outer[:, b * size : (b + 1) * size]
        store(step).start()
        return carry

    lax.fori_loop(0, steps, body, 0)
    read = readout[...]
    scaling = lax.rsqrt(jnp.sum(read * read, axis=1, keepdims=True) / size + EPS)
    gate = packed_ref[:, 6 * size :]
    gated_ref[...] = (
        read * gain_ref[...].astype(jnp.float32) * (gate / (1.0 + jnp.exp(-gate)))
    ).astype(jnp.bfloat16)
    tall = jnp.broadcast_to(scaling, (total, 128))
    if total < 128:
        tall = jnp.concatenate([tall, jnp.zeros((128 - total, 128), jnp.float32)], axis=0)
    flat_ref[...] = tall.T[0:SMALL, 0:total].astype(jnp.bfloat16)
    for step in range(steps):
        store(step).wait()


def state_step(state, packed, head_gain):
    count, size, _ = state.shape
    steps = count // min(16, count)
    anywhere = pl.BlockSpec(memory_space=pl.ANY)
    return pl.pallas_call(
        state_kernel,
        in_specs=[anywhere, VMEM, VMEM],
        out_specs=[anywhere, VMEM, VMEM],
        out_shape=[
            jax.ShapeDtypeStruct(state.shape, state.dtype),
            jax.ShapeDtypeStruct((count, size), jnp.bfloat16),
            jax.ShapeDtypeStruct((SMALL, count), jnp.bfloat16),
        ],
        scratch_shapes=[
            pltpu.VMEM(state.shape, state.dtype),
            pltpu.VMEM((count, size), jnp.float32),
            pltpu.SemaphoreType.DMA((steps,)),
            pltpu.SemaphoreType.DMA((steps,)),
        ],
    )(state, packed, head_gain.reshape(1, size))


def output_kernel(
    heads,
    groups,
    stream_ref,
    gated_ref,
    scaling_ref,
    weight_hbm,
    out_ref,
    weight_ref,
    weight_sem,
    all_gated,
    all_scaling,
    columns,
    held,
    core_out,
    core_in,
    hop_out,
    hop_in,
    gated_send,
    gated_recv,
    scaling_send,
    scaling_recv,
    core_send,
    core_recv,
    hop_send,
    hop_recv,
):
    me = lax.axis_index("tp")
    place = me % heads
    group = me // heads
    rows, cols = stream_ref.shape
    batch = all_gated.shape[0]
    group_rows = batch // groups
    dims = heads.bit_length() - 2
    chips = 1 << dims
    sibling = flip(me, (0,))
    neighbours = [flip(me, (bit,)) for bit in range(1, dims + 1)]
    others = [place + heads * ((group + j) % groups) for j in range(1, groups)]
    weight_copy = pltpu.make_async_copy(weight_hbm, weight_ref, weight_sem)
    weight_copy.start()
    enter([sibling] + neighbours + others)
    own_rows = pl.ds(pl.multiple_of(group * group_rows, group_rows), group_rows)
    copies = []
    arriving = []
    for j in range(1, groups):
        for source, target, send, recv in (
            (gated_ref, all_gated.at[own_rows], gated_send, gated_recv),
            (scaling_ref, all_scaling.at[group], scaling_send, scaling_recv),
        ):
            copy = remote(source, target, send.at[j - 1], recv.at[j - 1], others[j - 1])
            copy.start()
            copies.append(copy)
    all_gated[own_rows, :] = gated_ref[...]
    all_scaling[group] = scaling_ref[...]
    for copy in copies:
        copy.wait_recv()
    weight_copy.wait()
    wide = max(group_rows, 128)
    for g in range(groups):
        flat = all_scaling[g].astype(jnp.float32)
        if wide > group_rows:
            flat = jnp.concatenate(
                [flat, jnp.zeros((SMALL, wide - group_rows), jnp.float32)], axis=1
            )
        flat = jnp.concatenate([flat, jnp.zeros((128 - SMALL, wide), jnp.float32)], axis=0)
        columns[g * group_rows : (g + 1) * group_rows, :] = flat.T[0:group_rows]

    def relative(owner, mask):
        bits = tuple(bit for bit in range(1, dims + 1) if mask >> (bit - 1) & 1)
        begin = flip(owner, bits) * rows
        return pl.ds(pl.multiple_of(begin, rows), rows)

    def head_rows(owner, masks):
        picks = [relative(owner, mask) for mask in masks]
        left = jnp.concatenate([all_gated[pick, :] for pick in picks], axis=0)
        scale = jnp.concatenate([columns[pick, 0:1] for pick in picks], axis=0)
        product = lax.dot_general(
            left, weight_ref[...], (((1,), (1,)), ((), ())), preferred_element_type=jnp.float32
        )
        return product * scale

    core_copies = [
        remote(
            core_out.at[mask], core_in.at[mask], core_send.at[mask], core_recv.at[mask], sibling
        )
        for mask in range(chips)
    ]
    batch_of = min(4, chips)
    sweep = list(range(chips - 1, -1, -1))
    for first in range(0, chips, batch_of):
        masks = sweep[first : first + batch_of]
        product = head_rows(flip(place, (0,)), masks).astype(jnp.bfloat16)
        for i, mask in enumerate(masks):
            core_out[mask] = product[i * rows : (i + 1) * rows]
            core_copies[mask].start()
    for first in range(0, chips, batch_of):
        masks = sweep[first : first + batch_of]
        product = head_rows(place, masks)
        for i, mask in enumerate(masks):
            held[mask] = product[i * rows : (i + 1) * rows]

    parts = parts_of(cols, dims)
    hops = []
    waiting = [[] for _ in range(dims)]

    def cross(step, p, mask):
        (start, width), order = parts[p]
        if step == dims or not mask >> (order[step] - 1) & 1:
            return
        span = pl.ds(start, width)
        landed = mask - (1 << (order[step] - 1))
        hop_out[step, landed, :, span] = held[mask, :, span].astype(jnp.bfloat16)
        copy = remote(
            hop_out.at[step, landed, :, span],
            hop_in.at[step, landed, :, span],
            hop_send.at[step, p, landed],
            hop_recv.at[step, p, landed],
            neighbours[order[step] - 1],
        )
        copy.start()
        hops.append(copy)
        waiting[step].append((p, landed, span, copy))

    for mask in sweep:
        core_copies[mask].wait_recv()
        held[mask] += core_in[mask].astype(jnp.float32)
        for p in range(len(parts)):
            cross(0, p, mask)
    for step in range(dims):
        for p, landed, span, copy in waiting[step]:
            copy.wait_recv()
            held[landed, :, span] += hop_in[step, landed, :, span].astype(jnp.float32)
            cross(step + 1, p, landed)
    out_ref[...] = (stream_ref[...].astype(jnp.float32) + held[0]).astype(jnp.bfloat16)
    for copy in copies + core_copies + hops:
        copy.wait_send()


def output(stream, gated, scaling, out_weight, heads, groups):
    rows, cols = stream.shape
    batch = rows * heads
    group_rows, size = gated.shape
    dims = heads.bit_length() - 2
    chips = 1 << dims
    parts = len(parts_of(cols, dims))
    extra = groups - 1
    dma = pltpu.SemaphoreType.DMA
    anywhere = pl.BlockSpec(memory_space=pl.ANY)
    return pl.pallas_call(
        functools.partial(output_kernel, heads, groups),
        in_specs=[VMEM] * 3 + [anywhere],
        out_specs=VMEM,
        out_shape=jax.ShapeDtypeStruct(stream.shape, stream.dtype),
        scratch_shapes=[
            pltpu.VMEM(out_weight.shape, out_weight.dtype),
            dma(()),
            pltpu.VMEM((batch, size), jnp.bfloat16),
            pltpu.VMEM((groups, SMALL, group_rows), jnp.bfloat16),
            pltpu.VMEM((batch, 128), jnp.float32),
            pltpu.VMEM((chips, rows, cols), jnp.float32),
            pltpu.VMEM((chips, rows, cols), jnp.bfloat16),
            pltpu.VMEM((chips, rows, cols), jnp.bfloat16),
            pltpu.VMEM((dims, chips, rows, cols), jnp.bfloat16),
            pltpu.VMEM((dims, chips, rows, cols), jnp.bfloat16),
            dma((extra,)),
            dma((extra,)),
            dma((extra,)),
            dma((extra,)),
            dma((chips,)),
            dma((chips,)),
            dma((dims, parts, chips)),
            dma((dims, parts, chips)),
        ],
        compiler_params=pltpu.CompilerParams(
            collective_id=1, has_side_effects=True
        ),
    )(stream, gated, scaling, out_weight)


def masked(mask, dims):
    return tuple(bit for bit in range(1, dims + 1) if mask >> (bit - 1) & 1)


def fused_kernel(
    heads,
    groups,
    stream_hbm,
    gain_hbm,
    query_w,
    key_w,
    value_w,
    gate_w,
    write_w,
    decay_w,
    rate_hbm,
    head_gain_hbm,
    out_w,
    state_ref,
    held,
    mine_out,
    rise_out,
    stream_ref,
    gain_ref,
    rate_ref,
    head_gain_ref,
    gathered,
    weights,
    side_w,
    wide_side,
    side_rows,
    gain_row,
    gains,
    four_w,
    partial,
    partial_side,
    sent,
    received,
    small_sent,
    small_received,
    packed,
    answers,
    gated,
    left,
    acc,
    hop_out,
    hop_in,
    local_sems,
    state_sems,
    pair_sems,
    send_sems,
    ici_recv,
    core_recv,
    main_recv,
    small_recv,
    gated_recv,
    hop_recv,
):
    me = lax.axis_index("tp")
    place = me % heads
    group = me // heads
    core = place % 2
    rows, cols = stream_ref.shape
    size = query_w.shape[1]
    dims = heads.bit_length() - 2
    chips = 1 << dims
    flats = chips // 2
    chip_rows = 2 * rows
    group_rows = flats * chip_rows
    count = 16
    x, y, z = 1, 2, flats
    sibling = flip(me, (0,))
    neighbours = [flip(me, (bit,)) for bit in range(1, dims + 1)]
    partner = place + heads * ((group + 1) % groups)
    peers = [sibling] + neighbours + [partner, flip(partner, (0,))]
    for h in range(2):
        there = flip(partner, (h + 1,))
        peers += [flip(neighbours[h], (0,)), there, flip(there, (0,))]
    own_cols = pl.ds(pl.multiple_of(group * cols, cols), cols)
    upper = place // flats // 2
    keep = (upper + group) % 2
    outer = 1 - keep

    barrier = pltpu.get_barrier_semaphore()
    for device in peers:
        pl.semaphore_signal(barrier, inc=1, device_id=(device,), device_id_type=MESH)
    early = [
        pltpu.make_async_copy(source, target, local_sems.at[i])
        for i, (source, target) in enumerate(
            (
                (stream_hbm, stream_ref),
                (gain_hbm, gain_ref),
                (rate_hbm, rate_ref),
                (head_gain_hbm, head_gain_ref),
            )
        )
    ]
    for copy in early:
        copy.start()
    for i, weight in enumerate((query_w, key_w, value_w, gate_w)):
        pltpu.make_async_copy(
            weight, weights.at[:, i * size : (i + 1) * size], local_sems.at[4]
        ).start()
    for i, source in enumerate((write_w, decay_w)):
        pltpu.make_async_copy(
            source.at[:, own_cols], side_w.at[i * heads : (i + 1) * heads], local_sems.at[5]
        ).start()
    weights_done = pltpu.make_async_copy(weights, weights, local_sems.at[4])
    side_done = pltpu.make_async_copy(side_w, side_w, local_sems.at[5])
    own_w = pltpu.make_async_copy(out_w, four_w.at[:, 0:size], local_sems.at[6])
    sibling_w = remote(
        out_w, four_w.at[:, size : 2 * size], pair_sems.at[0], pair_sems.at[1], sibling
    )
    pieces = 4
    wide_half = cols // 2
    tall = wide_half // pieces

    def beside_w(h, i, n=1):
        spot = slice(h * wide_half + i * tall, h * wide_half + (i + n) * tall)
        return remote(
            out_w.at[spot, :],
            four_w.at[spot, 2 * size : 3 * size],
            pair_sems.at[3],
            pair_sems.at[4 + i],
            neighbours[h],
        )

    def passed_w(h, i):
        spot = slice(h * wide_half + i * tall, h * wide_half + (i + 1) * tall)
        return remote(
            four_w.at[spot, 2 * size : 3 * size],
            four_w.at[spot, 3 * size : 4 * size],
            pair_sems.at[2],
            pair_sems.at[4 + pieces],
            sibling,
        )

    def far_w(rows_of):
        target = four_w.at[0:rows_of, 2 * size : 3 * size]
        return target, target

    def fetch(c):
        spot = pl.ds(pl.multiple_of(c * chip_rows, chip_rows), chip_rows)
        return pltpu.make_async_copy(state_ref.at[spot], held.at[spot], state_sems.at[c])

    half = rows // 2
    top = dims
    parts = [(0, (top, 1, 2)), (half, (top, 2, 1))]

    def block(device_place, p, q):
        begin = device_place * rows + parts[p][0]
        return gathered.at[
            pl.ds(pl.multiple_of(begin, half), half), q * wide_half : (q + 1) * wide_half
        ]

    def pass_on(p, q, bits):
        order = parts[p][1]
        step = max([order.index(bit) for bit in bits], default=-1)
        target = block(flip(place, bits), p, q)
        source = target
        if not bits:
            source = stream_ref.at[
                parts[p][0] : parts[p][0] + half, q * wide_half : (q + 1) * wide_half
            ]
        for later in range(step + 1, dims):
            remote(
                source,
                target,
                send_sems.at[0],
                ici_recv.at[p, q, key_of(bits + (order[later],)) - 1],
                flip(me, (order[later],)),
            ).start()
        remote(source, target, send_sems.at[1], core_recv.at[key_of(bits)], sibling).start()

    def relay(p, q, mask):
        bits = masked(mask, dims)
        target = block(flip(place, bits), p, q)
        remote(target, target, send_sems.at[0], ici_recv.at[p, q, mask - 1], sibling).wait_recv()
        pass_on(p, q, bits)

    spot_x, spot_y = place // 2 % 2, place // 4 % 2

    def chip_of(c):
        return (spot_x + c) % 2 + 2 * ((spot_y + c // 2) % 2)

    def from_sibling(c, raised):
        level = (upper + raised) % 2
        begin = (level * flats + chip_of(c)) * chip_rows + (1 - core) * rows
        target = gathered.at[pl.ds(pl.multiple_of(begin, rows), rows), :]
        remote(
            target, target, send_sems.at[1], core_recv.at[c + flats * raised], sibling
        ).wait_recv()

    for copy in early:
        copy.wait()
    pl.semaphore_wait(barrier, len(peers))
    for q in range(2):
        for p in range(2):
            pass_on(p, q, ())
    sibling_w.start()
    gathered[pl.ds(pl.multiple_of(place * rows, rows), rows), :] = stream_ref[...]
    gains[...] = gain_ref[...].astype(jnp.float32)
    tiles = cols // 128
    for i in range(tiles):
        gain_row[:, i * 128 : (i + 1) * 128] = gains[pl.ds(group * tiles + i, 1), :]
    side_done.wait()
    wide_side[...] = side_w[...].astype(jnp.float32)
    for i in range(2):
        side_rows[i : i + 1, :] = wide_side[pl.ds(i * heads + place, 1), :]
    weights_done.wait()
    for c in range(flats):
        fetch(chip_of(c)).start()
    own_w.start()

    def project(begin, high):
        x = gathered[pl.ds(pl.multiple_of(begin, chip_rows), high), :].astype(jnp.float32)
        gained = (x * gain_row[...]).astype(jnp.bfloat16)
        product = jnp.dot(gained, weights[...], preferred_element_type=jnp.float32)
        exact = gained.astype(jnp.float32)
        write = jnp.sum(exact * side_rows[0:1, :], axis=1, keepdims=True)
        decay = jnp.sum(exact * side_rows[1:2, :], axis=1, keepdims=True)
        squares = jnp.sum(x * x, axis=1, keepdims=True)
        lane = lax.broadcasted_iota(jnp.int32, (high, 128), 1)
        side = jnp.where(
            lane == 0, write, jnp.where(lane == 1, decay, jnp.where(lane == 2, squares, 0.0))
        )
        return product, side

    away_begin = (group + 1) % groups * group_rows

    def main_copy(c):
        return remote(sent.at[c], received.at[c], send_sems.at[2], main_recv.at[c], partner)

    def small_copy(c):
        return remote(
            small_sent.at[c], small_received.at[c], send_sems.at[3], small_recv.at[c], partner
        )

    def project_away(c, raised, send=True):
        from_sibling(c, raised)
        product, side = project(away_begin + chip_of(c) * chip_rows, chip_rows)
        sent[c] = product.astype(jnp.bfloat16)
        if chip_rows < 128:
            side = jnp.concatenate(
                [side, jnp.zeros((128 - chip_rows, 128), jnp.float32)], axis=0
            )
        small_sent[c] = side.T[0:TINY].astype(jnp.bfloat16)
        if send:
            send_away(c)

    def send_away(c):
        main_copy(c).start()
        small_copy(c).start()

    def project_here(j, raised):
        for c in range(2 * j, 2 * j + 2):
            from_sibling(c, raised)
        pair = (spot_y + j) % 2
        spot = pl.ds(pl.multiple_of(pair * 2 * chip_rows, 2 * chip_rows), 2 * chip_rows)
        product, side = project(group * group_rows + pair * 2 * chip_rows, 2 * chip_rows)
        partial[spot, :] = product
        partial_side[spot, :] = side

    def marks(n):
        return lax.broadcasted_iota(jnp.int32, (n * count, size), 0) % count

    def diagonal(values, spots):
        return jnp.concatenate(
            [jnp.where(spots == b, values, jnp.zeros_like(values)) for b in range(count)], axis=1
        )

    def rounded(v):
        return v.astype(jnp.bfloat16).astype(jnp.float32)

    mine = lax.broadcasted_iota(jnp.int32, rate_ref.shape, 1) == place
    rate = jnp.sum(jnp.where(mine, rate_ref[...], 0.0), axis=1, keepdims=True)

    def recall(c):
        main_copy(c).wait_recv()
        small_copy(c).wait_recv()
        begin = chip_of(c) * chip_rows
        whole = pl.ds(pl.multiple_of(begin, chip_rows), chip_rows)
        total = partial[whole, :] + received[c].astype(jnp.float32)
        flat = small_received[c].astype(jnp.float32)
        flat = jnp.concatenate([flat, jnp.zeros((128 - TINY, flat.shape[1]), jnp.float32)], axis=0)
        side = partial_side[whole, :] + flat.T[0:chip_rows]
        scale = lax.rsqrt(side[:, 2:3] / (cols * groups) + EPS)
        projected = rounded(total * scale)
        query = projected[:, :size]
        key = projected[:, size : 2 * size]
        query = query * lax.rsqrt(jnp.sum(query * query, axis=1, keepdims=True) + EPS) * size**-0.5
        key = key * lax.rsqrt(jnp.sum(key * key, axis=1, keepdims=True) + EPS)
        key_high, key_low = split(key)
        query_high, query_low = split(query)
        fetch(chip_of(c)).wait()
        spots = marks(4)
        for i in range(chip_rows // count):
            near = slice(i * count, (i + 1) * count)
            spot = pl.ds(pl.multiple_of(begin + i * count, count), count)
            four = [v[near] for v in (key_high, key_low, query_high, query_low)]
            wide = diagonal(jnp.concatenate(four, axis=0), spots)
            memory = held[spot].reshape(count * size, size).astype(jnp.bfloat16)
            both = jnp.dot(wide, memory, preferred_element_type=jnp.float32)
            answers[0, near, :] = both[0:count] + both[count : 2 * count]
            answers[1, near, :] = both[2 * count : 3 * count] + both[3 * count : 4 * count]
        pre = rounded(side * scale)
        strength = jax.nn.sigmoid(pre[:, 0:1])
        decay = pre[:, 1:2]
        softplus = jnp.maximum(decay, 0.0) + jnp.log(1.0 + jnp.exp(-jnp.abs(decay)))
        factor = jnp.broadcast_to(jnp.exp(-rate * softplus), (chip_rows, size))
        overlap = jnp.sum(query * key, axis=1, keepdims=True)
        gate = projected[:, 3 * size :]
        lift = head_gain_ref[...].astype(jnp.float32) * (gate / (1.0 + jnp.exp(-gate)))
        change = strength * (projected[:, 2 * size : 3 * size] - factor * answers[0])
        read = factor * answers[1] + overlap * change
        scaling = lax.rsqrt(jnp.sum(read * read, axis=1, keepdims=True) / size + EPS)
        gated[c] = (read * scaling * lift).astype(jnp.bfloat16)
        same = gated.at[c, pl.ds(pl.multiple_of(core * rows, rows), rows), :]
        cross = gated.at[c, pl.ds(pl.multiple_of((1 - core) * rows, rows), rows), :]
        for h in range(2 if c else 1):
            gap, row = (c // 2, c % 2) if h else (c % 2, c // 2)
            span = slice(row * rows, (row + 1) * rows)
            first = 2 * gap
            there = flip(partner, (h + 1,)) if gap else partner
            here = neighbours[h] if gap else me
            for source, phase, j, device in (
                (same, 1, first, there),
                (cross, 1, first + 1, flip(there, (0,))),
                (cross, 0, first + 1, flip(here, (0,))),
                (same, 0, first, here),
            ):
                target = left.at[h, phase, span, j * size : (j + 1) * size]
                if phase or j:
                    remote(source, target, send_sems.at[4], gated_recv.at[h, phase], device).start()
                else:
                    left[h, 0, span, 0:size] = gated[
                        c, pl.ds(pl.multiple_of(core * rows, rows), rows), :
                    ]
        packed[c, 0] = key
        packed[c, 1] = change
        packed[c, 2] = factor

    def update(c):
        begin = chip_of(c) * chip_rows
        spots = marks(3)

        def body(i, carry):
            near = pl.ds(pl.multiple_of(i * count, count), count)
            key_high, key_low = split(packed[c, 0, near, :])
            change_high, change_low = split(packed[c, 1, near, :])
            factor = packed[c, 2, near, :]
            keys = jnp.concatenate([key_high, key_low, key_high], axis=0)
            keys = jnp.concatenate([keys, jnp.zeros((size - 3 * count, size), keys.dtype)], axis=0)
            keys = keys.astype(jnp.float32).T.astype(jnp.bfloat16)[:, 0 : 3 * count]
            wide = diagonal(jnp.concatenate([change_high, change_high, change_low], axis=0), spots)
            outer_product = jnp.dot(keys, wide, preferred_element_type=jnp.float32)
            for b in range(count):
                spot = begin + i * count + b
                held[spot] = (
                    factor[b : b + 1, :] * held[spot]
                    + outer_product[:, b * size : (b + 1) * size]
                )
            return carry

        lax.fori_loop(0, chip_rows // count, body, 0)

    def hop(phase, h, k):
        return remote(
            hop_out.at[phase, h, k],
            hop_in.at[phase, h, k],
            send_sems.at[5],
            hop_recv.at[phase, h, k],
            neighbours[1 - h],
        )

    slim = wide_half // 2

    def expand(phase):
        lefts = [left[0, phase], left[1, phase]]
        upper_rows = jnp.concatenate(
            [lefts[0][0:rows, 0 : 2 * size], lefts[1][0:rows, 2 * size :]], axis=1
        )
        lefts[1] = jnp.concatenate([upper_rows, lefts[1][rows:]], axis=0)
        for k in range(2):
            for h in range(2):
                begin = h * wide_half + k * slim
                span = slice(begin, begin + slim)
                product = lax.dot_general(
                    lefts[h],
                    four_w[span, :],
                    (((1,), (1,)), ((), ())),
                    preferred_element_type=jnp.float32,
                )
                hop_out[phase, h, k] = product[rows:].astype(jnp.bfloat16)
                hop(phase, h, k).start()
                acc[phase, :, span] = product[0:rows]

    def settle(phase):
        for k in range(2):
            for h in range(2):
                begin = h * wide_half + k * slim
                span = slice(begin, begin + slim)
                hop(phase, h, k).wait_recv()
                total = acc[phase, :, span] + hop_in[phase, h, k].astype(jnp.float32)

                @pl.when(keep == phase)
                def _():
                    mine_out[:, span] = total

                @pl.when(keep != phase)
                def _():
                    rise_out[:, span] = total.astype(jnp.bfloat16)

    def gated_bytes(h, phase):
        blocks = (6, 8) if h == 0 else (5, 6)
        return gathered.at[0:rows, 0 : blocks[phase] * size]

    def whole_left(phase):
        for h in range(2):
            target = gated_bytes(h, phase)
            remote(target, target, send_sems.at[4], gated_recv.at[h, phase], sibling).wait_recv()

    def relays(masks, halves=(0, 1)):
        for q in halves:
            for p, mask in masks:
                relay(p, q, mask)

    def send_beside(first, last):
        for i in range(first, last):
            for h in range(2):
                beside_w(h, i).start()

    def pass_weights(i):
        remote(*far_w(2 * tall), pair_sems.at[3], pair_sems.at[4 + i], sibling).wait_recv()
        for h in range(2):
            passed_w(h, i).start()

    def weights_ready():
        own_w.wait()
        sibling_w.wait_recv()
        remote(*far_w(cols), pair_sems.at[3], pair_sems.at[4 + pieces], sibling).wait_recv()

    def drain():
        sibling_w.wait_send()
        for i in range(2, 4):
            remote(*far_w(cols), pair_sems.at[i], pair_sems.at[4], sibling).wait_send()
        ici_rows = rows * (chips - 1)
        for i, ref in enumerate(
            (gathered.at[0:ici_rows, :], gathered.at[0 : rows * chips, :], sent, small_sent)
        ):
            remote(ref, ref, send_sems.at[i], main_recv.at[0], partner).wait_send()
        for phase in range(2):
            for h in range(2):
                target = gated_bytes(h, phase)
                remote(target, target, send_sems.at[4], gated_recv.at[0, 0], sibling).wait_send()
        remote(hop_out, hop_in, send_sems.at[5], hop_recv.at[0, 0, 0], sibling).wait_send()

    @pl.when(outer == 1)
    def _():
        relays([(0, z), (1, z)])
        project_away(0, 1)
        relays([(0, x + z), (1, y + z), (1, x + z), (0, y + z)])
        relays([(0, x), (1, y), (1, x), (0, y)])
        send_beside(0, pieces)
        project_away(1, 1)
        project_away(2, 1)
        project_here(0, 0)
        relays([(0, x + y + z), (1, x + y + z)])
        project_away(3, 1)
        relays([(0, x + y), (1, x + y)])
        project_here(1, 0)

    @pl.when(outer == 0)
    def _():
        project_away(0, 0, False)
        relays([(0, x), (1, y), (1, x), (0, y)], (0,))
        send_away(0)
        relays([(0, x), (1, y), (1, x), (0, y)], (1,))
        project_away(1, 0)
        project_away(2, 0)
        relays([(0, z), (1, z)])
        send_beside(0, 1)
        relays([(0, x + y), (1, x + y)])
        project_away(3, 0)
        relays([(0, x + z), (1, y + z), (1, x + z), (0, y + z)])
        send_beside(1, pieces)
        project_here(0, 1)
        relays([(0, x + y + z), (1, x + y + z)])
        project_here(1, 1)

    recall(0)
    recall(1)
    pass_weights(0)
    recall(2)
    pass_weights(1)
    pass_weights(2)
    pass_weights(3)
    recall(3)
    update(0)
    weights_ready()
    whole_left(0)
    expand(0)
    update(1)
    whole_left(1)
    expand(1)
    update(2)
    update(3)
    settle(0)
    settle(1)
    drain()


def fused(
    stream,
    norm_gain,
    weights,
    write_weight,
    decay_weight,
    rate,
    head_gain,
    out_weight,
    state,
    groups,
):
    rows, cols = stream.shape
    heads = rate.shape[0]
    size = weights[0].shape[1]
    chips = heads // 2
    flats = chips // 2
    batch = rows * heads
    chip_rows = 2 * rows
    dma = pltpu.SemaphoreType.DMA
    anywhere = pl.BlockSpec(memory_space=pltpu.HBM)
    f32, bf16 = jnp.float32, jnp.bfloat16
    return pl.pallas_call(
        functools.partial(fused_kernel, heads, groups),
        in_specs=[anywhere] * 12,
        out_specs=[VMEM] * 3,
        out_shape=[
            pltpu.VMEM(state.shape, state.dtype),
            pltpu.VMEM(stream.shape, f32),
            pltpu.VMEM(stream.shape, bf16),
        ],
        scratch_shapes=[
            pltpu.VMEM(stream.shape, stream.dtype),
            pltpu.VMEM((groups * cols // 128, 128), bf16),
            pltpu.VMEM((1, heads), f32),
            pltpu.VMEM((1, size), bf16),
            pltpu.VMEM((batch, cols), bf16),
            pltpu.VMEM((cols, 4 * size), bf16),
            pltpu.VMEM((2 * heads, cols), bf16),
            pltpu.VMEM((2 * heads, cols), f32),
            pltpu.VMEM((2, cols), f32),
            pltpu.VMEM((1, cols), f32),
            pltpu.VMEM((groups * cols // 128, 128), f32),
            pltpu.VMEM((cols, 4 * size), bf16),
            pltpu.VMEM((flats * chip_rows, 4 * size), f32),
            pltpu.VMEM((flats * chip_rows, 128), f32),
            pltpu.VMEM((flats, chip_rows, 4 * size), bf16),
            pltpu.VMEM((flats, chip_rows, 4 * size), bf16),
            pltpu.VMEM((flats, TINY, max(128, chip_rows)), bf16),
            pltpu.VMEM((flats, TINY, max(128, chip_rows)), bf16),
            pltpu.VMEM((flats, 3, chip_rows, size), f32),
            pltpu.VMEM((2, chip_rows, size), f32),
            pltpu.VMEM((flats, chip_rows, size), bf16),
            pltpu.VMEM((2, 2, 2 * rows, 4 * size), bf16),
            pltpu.VMEM((2, rows, cols), f32),
            pltpu.VMEM((2, 2, 2, rows, cols // 4), bf16),
            pltpu.VMEM((2, 2, 2, rows, cols // 4), bf16),
            dma((7,)),
            dma((flats,)),
            dma((9,)),
            dma((6,)),
            dma((2, 2, chips - 1)),
            dma((chips,)),
            dma((flats,)),
            dma((flats,)),
            dma((2, 2)),
            dma((2, 2, 2)),
        ],
        compiler_params=pltpu.CompilerParams(
            collective_id=2, has_side_effects=True, vmem_limit_bytes=43 << 20
        ),
    )(
        stream,
        norm_gain.reshape(groups * cols // 128, 128),
        *weights,
        write_weight.T,
        decay_weight.T,
        rate.reshape(1, heads),
        head_gain.reshape(1, size),
        out_weight,
        state,
    )


def store_kernel(held, new_ref, sems):
    steps = sems.shape[0]
    count = held.shape[0] // steps
    copies = []
    for step in range(steps):
        spot = slice(step * count, (step + 1) * count)
        copies.append(pltpu.make_async_copy(held.at[spot], new_ref.at[spot], sems.at[step]))
        copies[-1].start()
    for copy in copies:
        copy.wait()


def store(held):
    steps = min(8, held.shape[0])
    return pl.pallas_call(
        store_kernel,
        in_specs=[VMEM],
        out_specs=pl.BlockSpec(memory_space=pl.ANY),
        out_shape=jax.ShapeDtypeStruct(held.shape, held.dtype),
        scratch_shapes=[pltpu.SemaphoreType.DMA((steps,))],
        cost_estimate=pl.CostEstimate(
            flops=1000 * held.size, bytes_accessed=4 * held.size, transcendentals=0
        ),
        compiler_params=pltpu.CompilerParams(vmem_limit_bytes=4 << 20),
    )(held)


def per_device(
    stream,
    norm_gain,
    query_weight,
    key_weight,
    value_weight,
    gate_weight,
    write_weight,
    decay_weight,
    decay_rate,
    head_gain,
    out_weight,
    state,
):
    heads = decay_rate.shape[0]
    groups = lax.axis_size("tp") // heads
    weights = (query_weight, key_weight, value_weight, gate_weight)
    rows, cols = stream.shape
    if groups == 2 and heads == 16 and rows % 32 == 0 and rows <= 64 and cols % 256 == 0:
        held, mine, rise = fused(
            stream,
            norm_gain,
            weights,
            write_weight,
            decay_weight,
            decay_rate,
            head_gain,
            out_weight,
            state,
            groups,
        )
        span = heads // 2
        pairs = [
            (i, i + span * (1 - 2 * (i // span % 2))) for i in range(lax.axis_size("tp"))
        ]
        arrived = lax.ppermute(rise, "tp", pairs)
        updated = store(held)
        result = stream.astype(jnp.float32) + mine + arrived.astype(jnp.float32)
        return (result.astype(stream.dtype), updated)
    packed = project(
        stream, norm_gain, weights, write_weight, decay_weight, decay_rate, heads, groups
    )
    updated, gated, scaling = state_step(state, packed, head_gain)
    result = output(stream, gated, scaling, out_weight, heads, groups)
    return (result, updated)


def solution(mesh):
    placed = (
        P("tp", None),
        P(),
        P("tp", None),
        P("tp", None),
        P("tp", None),
        P("tp", None),
        P(),
        P(),
        P(),
        P(),
        P("tp", None),
        P("tp", None, None),
    )
    return jax.shard_map(
        per_device,
        mesh=mesh,
        in_specs=placed,
        out_specs=(P("tp", None), P("tp", None, None)),
        check_vma=False,
    )
```

```python
import functools

import jax
import jax.numpy as jnp
from jax import lax
from jax.experimental import pallas as pl
from jax.experimental.pallas import tpu as pltpu
from jax.sharding import PartitionSpec as P

EPS = 1e-06
MESH = pl.DeviceIdType.MESH
VMEM = pl.BlockSpec(memory_space=pltpu.VMEM)
SMALL = 16
TINY = 8


def flip(me, bits):
    other = me
    for bit in bits:
        other = other + (1 - 2 * ((me // (1 << bit)) % 2)) * (1 << bit)
    return other


def parts_of(cols, dims):
    tiles = cols // 128
    count = max(1, min(dims, tiles))
    cuts = [tiles * i // count * 128 for i in range(count + 1)]
    ranges = [(cuts[i], cuts[i + 1] - cuts[i]) for i in range(count)]
    orders = [[1 + (i + j) % dims for j in range(dims)] for i in range(count)]
    return list(zip(ranges, orders))


def masks_of(order):
    sets = [((), -1)]
    for step in range(len(order)):
        sets = sets + [(bits + (order[step],), step) for bits, _ in sets]
    return sets


def key_of(bits):
    return sum(1 << (bit - 1) for bit in bits)


def enter(devices):
    barrier = pltpu.get_barrier_semaphore()
    for device in devices:
        pl.semaphore_signal(barrier, inc=1, device_id=(device,), device_id_type=MESH)
    pl.semaphore_wait(barrier, len(devices))


def remote(source, target, send_sem, recv_sem, device):
    return pltpu.make_async_remote_copy(
        src_ref=source,
        dst_ref=target,
        send_sem=send_sem,
        recv_sem=recv_sem,
        device_id=(device,),
        device_id_type=MESH,
    )


def project_kernel(
    heads,
    groups,
    stream_ref,
    gain_ref,
    query_w,
    key_w,
    value_w,
    gate_w,
    write_w,
    decay_w,
    rate_ref,
    packed_out,
    gathered,
    weights,
    write_t,
    decay_t,
    gains,
    local_sems,
    partial,
    sent,
    received,
    small_sent,
    small_received,
    turned,
    ici_send,
    ici_recv,
    core_send,
    core_recv,
    group_send,
    group_recv,
    small_send,
    small_recv,
):
    me = lax.axis_index("tp")
    place = me % heads
    group = me // heads
    rows, cols = stream_ref.shape
    batch = gathered.shape[0]
    group_rows = batch // groups
    dims = heads.bit_length() - 2
    sibling = flip(me, (0,))
    neighbours = [flip(me, (bit,)) for bit in range(1, dims + 1)]
    others = [place + heads * ((group + j) % groups) for j in range(1, groups)]
    size = query_w.shape[1]
    own_cols = pl.ds(pl.multiple_of(group * cols, cols), cols)
    fetches = [
        pltpu.make_async_copy(
            weight, weights.at[:, i * size : (i + 1) * size], local_sems.at[i]
        )
        for i, weight in enumerate((query_w, key_w, value_w, gate_w))
    ] + [
        pltpu.make_async_copy(source.at[:, own_cols], target, local_sems.at[4 + i])
        for i, (source, target) in enumerate(((write_w, write_t), (decay_w, decay_t)))
    ]
    for fetch in fetches:
        fetch.start()
    enter([sibling] + neighbours + others)

    halves = 2 if rows % 32 == 0 and group_rows % rows == 0 else 1
    part_rows = rows // halves
    half_batch = batch // halves
    ranges = parts_of(cols, dims)

    def half_rows(h, device_place):
        begin = h * half_batch + device_place * part_rows
        return pl.ds(pl.multiple_of(begin, part_rows), part_rows)

    def block(h, device_place, part):
        return gathered.at[half_rows(h, device_place), pl.ds(part[0][0], part[0][1])]

    sends = []
    core_copies = [[] for _ in range(halves)]

    def pass_on(h, p, part, bits, step):
        order = part[1]
        origin = flip(place, bits)
        target = block(h, origin, part)
        if bits:
            source = target
        else:
            source = stream_ref.at[
                pl.ds(h * part_rows, part_rows), pl.ds(part[0][0], part[0][1])
            ]
        for later in range(step + 1, dims):
            landed = key_of(bits + (order[later],))
            copy = remote(
                source,
                target,
                ici_send.at[h, p, landed],
                ici_recv.at[h, p, landed],
                flip(me, (order[later],)),
            )
            copy.start()
            sends.append(copy)
        own = key_of(bits)
        copy = remote(source, target, core_send.at[h, p, own], core_recv.at[h, p, own], sibling)
        copy.start()
        core_copies[h].append(copy)

    def begin(h):
        for p, part in enumerate(ranges):
            pass_on(h, p, part, (), -1)

    def relay(h, index):
        for p, part in enumerate(ranges):
            bits, step = masks_of(part[1])[index]
            landed = key_of(bits)
            target = block(h, flip(place, bits), part)
            remote(
                target, target, ici_send.at[h, p, landed], ici_recv.at[h, p, landed], sibling
            ).wait_recv()
            pass_on(h, p, part, bits, step)

    early = max(2, 1 << (dims - 1))
    begin(0)
    for h in range(halves):
        gathered[half_rows(h, place), :] = stream_ref[h * part_rows : (h + 1) * part_rows, :]
    relay(0, 1)
    for h in range(1, halves):
        begin(h)
    for index in range(2, 1 << dims):
        relay(0, index)
    for h in range(1, halves):
        for index in range(1, early):
            relay(h, index)
    for copy in core_copies[0]:
        copy.wait_recv()

    gains[...] = gain_ref[...].astype(jnp.float32)
    gain = jnp.concatenate(
        [gains[pl.ds(group * (cols // 128) + i, 1), :] for i in range(cols // 128)], axis=1
    )
    for fetch in fetches:
        fetch.wait()

    def project(begin, count, at):
        x = gathered[pl.ds(begin, count), :].astype(jnp.float32)
        gained = (x * gain).astype(jnp.bfloat16)
        partial[pl.ds(at, count), :] = jnp.dot(
            gained, weights[...], preferred_element_type=jnp.float32
        )
        mine = lax.broadcasted_iota(jnp.int32, (count, heads), 1) == place
        pre = [
            jnp.sum(
                jnp.where(
                    mine,
                    lax.dot_general(
                        gained,
                        w[...],
                        (((1,), (1,)), ((), ())),
                        preferred_element_type=jnp.float32,
                    ),
                    0.0,
                ),
                axis=1,
                keepdims=True,
            )
            for w in (write_t, decay_t)
        ]
        squares = jnp.sum(x * x, axis=1, keepdims=True)
        lane = lax.broadcasted_iota(jnp.int32, (count, 128), 1)
        return jnp.where(
            lane == 0, pre[0], jnp.where(lane == 1, pre[1], jnp.where(lane == 2, squares, 0.0))
        )

    copies = []
    wide = max(group_rows, 128)
    count = group_rows // halves

    def half_of(h, target_group):
        begin = h * half_batch + target_group * count
        return pl.multiple_of(begin, count)

    for h in range(halves):
        if h:
            for index in range(early, 1 << dims):
                relay(h, index)
            for copy in core_copies[h]:
                copy.wait_recv()
        for j in range(1, groups):
            spot = slice(h * count, (h + 1) * count)
            side = project(half_of(h, (group + j) % groups), count, 0)
            sent[j - 1, spot] = partial[0:count].astype(jnp.bfloat16)
            turned[spot] = side
            routes = [(sent.at[j - 1, spot], received.at[j - 1, spot], group_send, group_recv)]
            flat = turned[...].T
            small_sent[j - 1, :, spot] = flat[0:SMALL, spot].astype(jnp.bfloat16)
            routes.append(
                (
                    small_sent.at[j - 1, :, spot],
                    small_received.at[j - 1, :, spot],
                    small_send,
                    small_recv,
                )
            )
            for source, target, send, recv in routes:
                copy = remote(
                    source, target, send.at[h, j - 1], recv.at[h, j - 1], others[j - 1]
                )
                copy.start()
                copies.append(copy)
    for h in range(halves):
        turned[h * count : (h + 1) * count] = project(half_of(h, group), count, h * count)
    total = partial[...]
    flat = turned[...].T[0:SMALL, :]
    for copy in copies:
        copy.wait_recv()
    for j in range(1, groups):
        total = total + received[j - 1].astype(jnp.float32)
    small_total = flat[:, 0:group_rows]
    for j in range(1, groups):
        small_total = small_total + small_received[j - 1].astype(jnp.float32)
    turned_back = jnp.concatenate(
        [small_total, jnp.zeros((SMALL, wide - group_rows), jnp.float32)], axis=1
    ) if wide > group_rows else small_total
    side = jnp.concatenate(
        [turned_back, jnp.zeros((128 - SMALL, wide), jnp.float32)], axis=0
    ).T[0:group_rows]
    scale = lax.rsqrt(side[:, 2:3] / (cols * groups) + EPS)

    def rounded(v):
        return v.astype(jnp.bfloat16).astype(jnp.float32)

    projected = rounded(total * scale)
    query = projected[:, :size]
    key = projected[:, size : 2 * size]
    query = query * lax.rsqrt(jnp.sum(query * query, axis=1, keepdims=True) + EPS) * size**-0.5
    key = key * lax.rsqrt(jnp.sum(key * key, axis=1, keepdims=True) + EPS)
    pre = rounded(side * scale)
    strength = jax.nn.sigmoid(pre[:, 0:1])
    mine = lax.broadcasted_iota(jnp.int32, rate_ref.shape, 1) == place
    rate = jnp.sum(jnp.where(mine, rate_ref[...], 0.0), axis=1, keepdims=True)
    decay = pre[:, 1:2]
    softplus = jnp.maximum(decay, 0.0) + jnp.log(1.0 + jnp.exp(-jnp.abs(decay)))
    factor = jnp.exp(-rate * softplus)
    overlap = jnp.sum(query * key, axis=1, keepdims=True)
    results = [jnp.broadcast_to(v, (group_rows, size)) for v in (strength, factor, overlap)]
    results += [query, key, projected[:, 2 * size :]]
    for i, v in enumerate(results):
        span = pl.ds(i * size, v.shape[1])
        if halves == 1:
            packed_out[:, span] = v
            continue
        for h in range(halves):
            for q in range(group_rows // rows):
                to, come = q * rows + h * part_rows, h * count + q * part_rows
                packed_out[to : to + part_rows, span] = v[come : come + part_rows]
    for copy in sends + sum(core_copies, []) + copies:
        copy.wait_send()


def project(stream, norm_gain, weights, write_weight, decay_weight, rate, heads, groups):
    rows, cols = stream.shape
    batch = rows * heads
    group_rows = batch // groups
    size = weights[0].shape[1]
    dims = heads.bit_length() - 2
    parts = len(parts_of(cols, dims))
    extra = groups - 1
    halves = 2
    dma = pltpu.SemaphoreType.DMA
    anywhere = pl.BlockSpec(memory_space=pl.ANY)
    return pl.pallas_call(
        functools.partial(project_kernel, heads, groups),
        in_specs=[VMEM] * 2 + [anywhere] * 6 + [VMEM],
        out_specs=VMEM,
        out_shape=jax.ShapeDtypeStruct((group_rows, 7 * size), jnp.float32),
        scratch_shapes=[
            pltpu.VMEM((batch, cols), jnp.bfloat16),
            pltpu.VMEM((cols, 4 * size), jnp.bfloat16),
            pltpu.VMEM((heads, cols), jnp.bfloat16),
            pltpu.VMEM((heads, cols), jnp.bfloat16),
            pltpu.VMEM((groups * cols // 128, 128), jnp.float32),
            dma((6,)),
            pltpu.VMEM((group_rows, 4 * size), jnp.float32),
            pltpu.VMEM((extra, group_rows, 4 * size), jnp.bfloat16),
            pltpu.VMEM((extra, group_rows, 4 * size), jnp.bfloat16),
            pltpu.VMEM((extra, SMALL, group_rows), jnp.bfloat16),
            pltpu.VMEM((extra, SMALL, group_rows), jnp.bfloat16),
            pltpu.VMEM((max(group_rows, 128), 128), jnp.float32),
            dma((halves, parts, 1 << dims)),
            dma((halves, parts, 1 << dims)),
            dma((halves, parts, 1 << dims)),
            dma((halves, parts, 1 << dims)),
            dma((halves, extra)),
            dma((halves, extra)),
            dma((halves, extra)),
            dma((halves, extra)),
        ],
        compiler_params=pltpu.CompilerParams(
            collective_id=0, has_side_effects=True
        ),
    )(
        stream,
        norm_gain.reshape(groups * cols // 128, 128),
        *weights,
        write_weight.T,
        decay_weight.T,
        rate.reshape(1, heads),
    )


def split(v):
    high = v.astype(jnp.bfloat16)
    return high, (v - high.astype(jnp.float32)).astype(jnp.bfloat16)


def state_kernel(
    state_ref, packed_ref, gain_ref, new_ref, gated_ref, flat_ref, held, readout, in_sems, out_sems
):
    total, size, _ = state_ref.shape
    steps = in_sems.shape[0]
    count = total // steps

    def rows_of(step):
        return pl.ds(pl.multiple_of(step * count, count), count)

    def fetch(step):
        rows = rows_of(step)
        return pltpu.make_async_copy(state_ref.at[rows], held.at[rows], in_sems.at[step])

    def store(step):
        rows = rows_of(step)
        return pltpu.make_async_copy(held.at[rows], new_ref.at[rows], out_sems.at[step])

    for step in range(steps):
        fetch(step).start()
    spots = lax.broadcasted_iota(jnp.int32, (4 * count, size), 0) % count

    def diagonal(rows):
        marks = spots[0 : rows.shape[0]]
        return jnp.concatenate(
            [jnp.where(marks == b, rows, jnp.zeros_like(rows)) for b in range(count)], axis=1
        )

    def body(step, carry):
        rows = rows_of(step)

        def columns(first, width=1):
            return packed_ref[rows, first * size : (first + width) * size]

        key_high, key_low = split(columns(4))
        query_high, query_low = split(columns(3))
        four = jnp.concatenate([key_high, key_low, query_high, query_low], axis=0)
        strength, factor, overlap = columns(0), columns(1), columns(2)
        left = jnp.concatenate([key_high, key_low, key_high], axis=0)
        left = jnp.concatenate([left, jnp.zeros((size - 3 * count, size), left.dtype)], axis=0)
        left = left.astype(jnp.float32).T.astype(jnp.bfloat16)[:, 0 : 3 * count]
        wide = diagonal(four)
        fetch(step).wait()
        memory = held[rows].reshape(count * size, size).astype(jnp.bfloat16)
        both = jnp.dot(wide, memory, preferred_element_type=jnp.float32)
        recalled = both[0:count] + both[count : 2 * count]
        asked = both[2 * count : 3 * count] + both[3 * count : 4 * count]
        change = strength * (columns(5) - factor * recalled)
        readout[rows, :] = factor * asked + overlap * change
        change_high, change_low = split(change)
        right = diagonal(jnp.concatenate([change_high, change_high, change_low], axis=0))
        outer = jnp.dot(left, right, preferred_element_type=jnp.float32)
        for b in range(count):
            spot = step * count + b
            held[spot] = factor[b : b + 1, :] * held[spot] + outer[:, b * size : (b + 1) * size]
        store(step).start()
        return carry

    lax.fori_loop(0, steps, body, 0)
    read = readout[...]
    scaling = lax.rsqrt(jnp.sum(read * read, axis=1, keepdims=True) / size + EPS)
    gate = packed_ref[:, 6 * size :]
    gated_ref[...] = (
        read * gain_ref[...].astype(jnp.float32) * (gate / (1.0 + jnp.exp(-gate)))
    ).astype(jnp.bfloat16)
    tall = jnp.broadcast_to(scaling, (total, 128))
    if total < 128:
        tall = jnp.concatenate([tall, jnp.zeros((128 - total, 128), jnp.float32)], axis=0)
    flat_ref[...] = tall.T[0:SMALL, 0:total].astype(jnp.bfloat16)
    for step in range(steps):
        store(step).wait()


def state_step(state, packed, head_gain):
    count, size, _ = state.shape
    steps = count // min(16, count)
    anywhere = pl.BlockSpec(memory_space=pl.ANY)
    return pl.pallas_call(
        state_kernel,
        in_specs=[anywhere, VMEM, VMEM],
        out_specs=[anywhere, VMEM, VMEM],
        out_shape=[
            jax.ShapeDtypeStruct(state.shape, state.dtype),
            jax.ShapeDtypeStruct((count, size), jnp.bfloat16),
            jax.ShapeDtypeStruct((SMALL, count), jnp.bfloat16),
        ],
        scratch_shapes=[
            pltpu.VMEM(state.shape, state.dtype),
            pltpu.VMEM((count, size), jnp.float32),
            pltpu.SemaphoreType.DMA((steps,)),
            pltpu.SemaphoreType.DMA((steps,)),
        ],
    )(state, packed, head_gain.reshape(1, size))


def output_kernel(
    heads,
    groups,
    stream_ref,
    gated_ref,
    scaling_ref,
    weight_hbm,
    out_ref,
    weight_ref,
    weight_sem,
    all_gated,
    all_scaling,
    columns,
    held,
    core_out,
    core_in,
    hop_out,
    hop_in,
    gated_send,
    gated_recv,
    scaling_send,
    scaling_recv,
    core_send,
    core_recv,
    hop_send,
    hop_recv,
):
    me = lax.axis_index("tp")
    place = me % heads
    group = me // heads
    rows, cols = stream_ref.shape
    batch = all_gated.shape[0]
    group_rows = batch // groups
    dims = heads.bit_length() - 2
    chips = 1 << dims
    sibling = flip(me, (0,))
    neighbours = [flip(me, (bit,)) for bit in range(1, dims + 1)]
    others = [place + heads * ((group + j) % groups) for j in range(1, groups)]
    weight_copy = pltpu.make_async_copy(weight_hbm, weight_ref, weight_sem)
    weight_copy.start()
    enter([sibling] + neighbours + others)
    own_rows = pl.ds(pl.multiple_of(group * group_rows, group_rows), group_rows)
    copies = []
    arriving = []
    for j in range(1, groups):
        for source, target, send, recv in (
            (gated_ref, all_gated.at[own_rows], gated_send, gated_recv),
            (scaling_ref, all_scaling.at[group], scaling_send, scaling_recv),
        ):
            copy = remote(source, target, send.at[j - 1], recv.at[j - 1], others[j - 1])
            copy.start()
            copies.append(copy)
    all_gated[own_rows, :] = gated_ref[...]
    all_scaling[group] = scaling_ref[...]
    for copy in copies:
        copy.wait_recv()
    weight_copy.wait()
    wide = max(group_rows, 128)
    for g in range(groups):
        flat = all_scaling[g].astype(jnp.float32)
        if wide > group_rows:
            flat = jnp.concatenate(
                [flat, jnp.zeros((SMALL, wide - group_rows), jnp.float32)], axis=1
            )
        flat = jnp.concatenate([flat, jnp.zeros((128 - SMALL, wide), jnp.float32)], axis=0)
        columns[g * group_rows : (g + 1) * group_rows, :] = flat.T[0:group_rows]

    def relative(owner, mask):
        bits = tuple(bit for bit in range(1, dims + 1) if mask >> (bit - 1) & 1)
        begin = flip(owner, bits) * rows
        return pl.ds(pl.multiple_of(begin, rows), rows)

    def head_rows(owner, masks):
        picks = [relative(owner, mask) for mask in masks]
        left = jnp.concatenate([all_gated[pick, :] for pick in picks], axis=0)
        scale = jnp.concatenate([columns[pick, 0:1] for pick in picks], axis=0)
        product = lax.dot_general(
            left, weight_ref[...], (((1,), (1,)), ((), ())), preferred_element_type=jnp.float32
        )
        return product * scale

    core_copies = [
        remote(
            core_out.at[mask], core_in.at[mask], core_send.at[mask], core_recv.at[mask], sibling
        )
        for mask in range(chips)
    ]
    batch_of = min(4, chips)
    sweep = list(range(chips - 1, -1, -1))
    for first in range(0, chips, batch_of):
        masks = sweep[first : first + batch_of]
        product = head_rows(flip(place, (0,)), masks).astype(jnp.bfloat16)
        for i, mask in enumerate(masks):
            core_out[mask] = product[i * rows : (i + 1) * rows]
            core_copies[mask].start()
    for first in range(0, chips, batch_of):
        masks = sweep[first : first + batch_of]
        product = head_rows(place, masks)
        for i, mask in enumerate(masks):
            held[mask] = product[i * rows : (i + 1) * rows]

    parts = parts_of(cols, dims)
    hops = []
    waiting = [[] for _ in range(dims)]

    def cross(step, p, mask):
        (start, width), order = parts[p]
        if step == dims or not mask >> (order[step] - 1) & 1:
            return
        span = pl.ds(start, width)
        landed = mask - (1 << (order[step] - 1))
        hop_out[step, landed, :, span] = held[mask, :, span].astype(jnp.bfloat16)
        copy = remote(
            hop_out.at[step, landed, :, span],
            hop_in.at[step, landed, :, span],
            hop_send.at[step, p, landed],
            hop_recv.at[step, p, landed],
            neighbours[order[step] - 1],
        )
        copy.start()
        hops.append(copy)
        waiting[step].append((p, landed, span, copy))

    for mask in sweep:
        core_copies[mask].wait_recv()
        held[mask] += core_in[mask].astype(jnp.float32)
        for p in range(len(parts)):
            cross(0, p, mask)
    for step in range(dims):
        for p, landed, span, copy in waiting[step]:
            copy.wait_recv()
            held[landed, :, span] += hop_in[step, landed, :, span].astype(jnp.float32)
            cross(step + 1, p, landed)
    out_ref[...] = (stream_ref[...].astype(jnp.float32) + held[0]).astype(jnp.bfloat16)
    for copy in copies + core_copies + hops:
        copy.wait_send()


def output(stream, gated, scaling, out_weight, heads, groups):
    rows, cols = stream.shape
    batch = rows * heads
    group_rows, size = gated.shape
    dims = heads.bit_length() - 2
    chips = 1 << dims
    parts = len(parts_of(cols, dims))
    extra = groups - 1
    dma = pltpu.SemaphoreType.DMA
    anywhere = pl.BlockSpec(memory_space=pl.ANY)
    return pl.pallas_call(
        functools.partial(output_kernel, heads, groups),
        in_specs=[VMEM] * 3 + [anywhere],
        out_specs=VMEM,
        out_shape=jax.ShapeDtypeStruct(stream.shape, stream.dtype),
        scratch_shapes=[
            pltpu.VMEM(out_weight.shape, out_weight.dtype),
            dma(()),
            pltpu.VMEM((batch, size), jnp.bfloat16),
            pltpu.VMEM((groups, SMALL, group_rows), jnp.bfloat16),
            pltpu.VMEM((batch, 128), jnp.float32),
            pltpu.VMEM((chips, rows, cols), jnp.float32),
            pltpu.VMEM((chips, rows, cols), jnp.bfloat16),
            pltpu.VMEM((chips, rows, cols), jnp.bfloat16),
            pltpu.VMEM((dims, chips, rows, cols), jnp.bfloat16),
            pltpu.VMEM((dims, chips, rows, cols), jnp.bfloat16),
            dma((extra,)),
            dma((extra,)),
            dma((extra,)),
            dma((extra,)),
            dma((chips,)),
            dma((chips,)),
            dma((dims, parts, chips)),
            dma((dims, parts, chips)),
        ],
        compiler_params=pltpu.CompilerParams(
            collective_id=1, has_side_effects=True
        ),
    )(stream, gated, scaling, out_weight)


def masked(mask, dims):
    return tuple(bit for bit in range(1, dims + 1) if mask >> (bit - 1) & 1)


def renew(kept, read, write):
    count = 16
    _, total, size = kept.shape
    spots = lax.broadcasted_iota(jnp.int32, (3 * count, size), 0) % count

    def body(i, carry):
        near = pl.ds(pl.multiple_of(i * count, count), count)
        key_high, key_low = split(kept[0, near, :])
        change_high, change_low = split(kept[1, near, :])
        factor = kept[2, near, :]
        keys = jnp.concatenate([key_high, key_low, key_high], axis=0)
        keys = jnp.concatenate([keys, jnp.zeros((size - 3 * count, size), keys.dtype)], axis=0)
        keys = keys.astype(jnp.float32).T.astype(jnp.bfloat16)[:, 0 : 3 * count]
        changes = jnp.concatenate([change_high, change_high, change_low], axis=0)
        wide = jnp.concatenate(
            [jnp.where(spots == b, changes, jnp.zeros_like(changes)) for b in range(count)], axis=1
        )
        outer = jnp.dot(keys, wide, preferred_element_type=jnp.float32)
        for b in range(count):
            spot = i * count + b
            write(spot, factor[b : b + 1, :] * read(spot) + outer[:, b * size : (b + 1) * size])
        return carry

    lax.fori_loop(0, total // count, body, 0)


def fused_kernel(
    heads,
    groups,
    stream_hbm,
    gain_hbm,
    query_w,
    key_w,
    value_w,
    gate_w,
    write_w,
    decay_w,
    rate_hbm,
    head_gain_hbm,
    out_w,
    state_ref,
    held,
    mine_out,
    rise_out,
    late,
    stream_ref,
    gain_ref,
    rate_ref,
    head_gain_ref,
    gathered,
    weights,
    side_w,
    wide_side,
    side_rows,
    gain_row,
    gains,
    four_w,
    partial,
    partial_side,
    sent,
    received,
    small_sent,
    small_received,
    packed,
    answers,
    gated,
    left,
    acc,
    hop_out,
    hop_in,
    local_sems,
    state_sems,
    pair_sems,
    send_sems,
    ici_recv,
    core_recv,
    main_recv,
    small_recv,
    gated_recv,
    hop_recv,
):
    me = lax.axis_index("tp")
    place = me % heads
    group = me // heads
    core = place % 2
    rows, cols = stream_ref.shape
    size = query_w.shape[1]
    dims = heads.bit_length() - 2
    chips = 1 << dims
    flats = chips // 2
    chip_rows = 2 * rows
    group_rows = flats * chip_rows
    count = 16
    x, y, z = 1, 2, flats
    sibling = flip(me, (0,))
    neighbours = [flip(me, (bit,)) for bit in range(1, dims + 1)]
    partner = place + heads * ((group + 1) % groups)
    peers = [sibling] + neighbours + [partner, flip(partner, (0,))]
    for h in range(2):
        there = flip(partner, (h + 1,))
        peers += [flip(neighbours[h], (0,)), there, flip(there, (0,))]
    own_cols = pl.ds(pl.multiple_of(group * cols, cols), cols)
    upper = place // flats // 2
    keep = (upper + group) % 2
    outer = 1 - keep

    barrier = pltpu.get_barrier_semaphore()
    for device in peers:
        pl.semaphore_signal(barrier, inc=1, device_id=(device,), device_id_type=MESH)
    early = [
        pltpu.make_async_copy(source, target, local_sems.at[i])
        for i, (source, target) in enumerate(
            (
                (stream_hbm, stream_ref),
                (gain_hbm, gain_ref),
                (rate_hbm, rate_ref),
                (head_gain_hbm, head_gain_ref),
            )
        )
    ]
    for copy in early:
        copy.start()
    for i, weight in enumerate((query_w, key_w, value_w, gate_w)):
        pltpu.make_async_copy(
            weight, weights.at[:, i * size : (i + 1) * size], local_sems.at[4]
        ).start()
    for i, source in enumerate((write_w, decay_w)):
        pltpu.make_async_copy(
            source.at[:, own_cols], side_w.at[i * heads : (i + 1) * heads], local_sems.at[5]
        ).start()
    weights_done = pltpu.make_async_copy(weights, weights, local_sems.at[4])
    side_done = pltpu.make_async_copy(side_w, side_w, local_sems.at[5])
    own_w = pltpu.make_async_copy(out_w, four_w.at[:, 0:size], local_sems.at[6])
    sibling_w = remote(
        out_w, four_w.at[:, size : 2 * size], pair_sems.at[0], pair_sems.at[1], sibling
    )
    pieces = 4
    wide_half = cols // 2
    tall = wide_half // pieces

    def beside_w(h, i, n=1):
        spot = slice(h * wide_half + i * tall, h * wide_half + (i + n) * tall)
        return remote(
            out_w.at[spot, :],
            four_w.at[spot, 2 * size : 3 * size],
            pair_sems.at[3],
            pair_sems.at[4 + i],
            neighbours[h],
        )

    def passed_w(h, i):
        spot = slice(h * wide_half + i * tall, h * wide_half + (i + 1) * tall)
        return remote(
            four_w.at[spot, 2 * size : 3 * size],
            four_w.at[spot, 3 * size : 4 * size],
            pair_sems.at[2],
            pair_sems.at[4 + pieces],
            sibling,
        )

    def far_w(rows_of):
        target = four_w.at[0:rows_of, 2 * size : 3 * size]
        return target, target

    def fetch(c):
        spot = pl.ds(pl.multiple_of(c * chip_rows, chip_rows), chip_rows)
        return pltpu.make_async_copy(state_ref.at[spot], held.at[spot], state_sems.at[c])

    half = rows // 2
    top = dims
    parts = [(0, (top, 1, 2)), (half, (top, 2, 1))]

    def block(device_place, p, q):
        begin = device_place * rows + parts[p][0]
        return gathered.at[
            pl.ds(pl.multiple_of(begin, half), half), q * wide_half : (q + 1) * wide_half
        ]

    def pass_on(p, q, bits):
        order = parts[p][1]
        step = max([order.index(bit) for bit in bits], default=-1)
        target = block(flip(place, bits), p, q)
        source = target
        if not bits:
            source = stream_ref.at[
                parts[p][0] : parts[p][0] + half, q * wide_half : (q + 1) * wide_half
            ]
        for later in range(step + 1, dims):
            remote(
                source,
                target,
                send_sems.at[0],
                ici_recv.at[p, q, key_of(bits + (order[later],)) - 1],
                flip(me, (order[later],)),
            ).start()
        remote(source, target, send_sems.at[1], core_recv.at[key_of(bits)], sibling).start()

    def relay(p, q, mask):
        bits = masked(mask, dims)
        target = block(flip(place, bits), p, q)
        remote(target, target, send_sems.at[0], ici_recv.at[p, q, mask - 1], sibling).wait_recv()
        pass_on(p, q, bits)

    spot_x, spot_y = place // 2 % 2, place // 4 % 2

    def chip_of(c):
        return (spot_x + c) % 2 + 2 * ((spot_y + c // 2) % 2)

    def from_sibling(c, raised):
        level = (upper + raised) % 2
        begin = (level * flats + chip_of(c)) * chip_rows + (1 - core) * rows
        target = gathered.at[pl.ds(pl.multiple_of(begin, rows), rows), :]
        remote(
            target, target, send_sems.at[1], core_recv.at[c + flats * raised], sibling
        ).wait_recv()

    for copy in early:
        copy.wait()
    pl.semaphore_wait(barrier, len(peers))
    for q in range(2):
        for p in range(2):
            pass_on(p, q, ())
    sibling_w.start()
    gathered[pl.ds(pl.multiple_of(place * rows, rows), rows), :] = stream_ref[...]
    gains[...] = gain_ref[...].astype(jnp.float32)
    tiles = cols // 128
    for i in range(tiles):
        gain_row[:, i * 128 : (i + 1) * 128] = gains[pl.ds(group * tiles + i, 1), :]
    side_done.wait()
    wide_side[...] = side_w[...].astype(jnp.float32)
    for i in range(2):
        side_rows[i : i + 1, :] = wide_side[pl.ds(i * heads + place, 1), :]
    weights_done.wait()
    for c in range(flats):
        fetch(chip_of(c)).start()
    own_w.start()

    def project(begin, high):
        x = gathered[pl.ds(pl.multiple_of(begin, chip_rows), high), :].astype(jnp.float32)
        gained = (x * gain_row[...]).astype(jnp.bfloat16)
        product = jnp.dot(gained, weights[...], preferred_element_type=jnp.float32)
        exact = gained.astype(jnp.float32)
        write = jnp.sum(exact * side_rows[0:1, :], axis=1, keepdims=True)
        decay = jnp.sum(exact * side_rows[1:2, :], axis=1, keepdims=True)
        squares = jnp.sum(x * x, axis=1, keepdims=True)
        lane = lax.broadcasted_iota(jnp.int32, (high, 128), 1)
        side = jnp.where(
            lane == 0, write, jnp.where(lane == 1, decay, jnp.where(lane == 2, squares, 0.0))
        )
        return product, side

    away_begin = (group + 1) % groups * group_rows

    def main_copy(c):
        return remote(sent.at[c], received.at[c], send_sems.at[2], main_recv.at[c], partner)

    def small_copy(c):
        return remote(
            small_sent.at[c], small_received.at[c], send_sems.at[3], small_recv.at[c], partner
        )

    def project_away(c, raised, send=True):
        from_sibling(c, raised)
        product, side = project(away_begin + chip_of(c) * chip_rows, chip_rows)
        sent[c] = product.astype(jnp.bfloat16)
        if chip_rows < 128:
            side = jnp.concatenate(
                [side, jnp.zeros((128 - chip_rows, 128), jnp.float32)], axis=0
            )
        small_sent[c] = side.T[0:TINY].astype(jnp.bfloat16)
        if send:
            send_away(c)

    def send_away(c):
        main_copy(c).start()
        small_copy(c).start()

    def project_here(j, raised):
        for c in range(2 * j, 2 * j + 2):
            from_sibling(c, raised)
        pair = (spot_y + j) % 2
        spot = pl.ds(pl.multiple_of(pair * 2 * chip_rows, 2 * chip_rows), 2 * chip_rows)
        product, side = project(group * group_rows + pair * 2 * chip_rows, 2 * chip_rows)
        partial[spot, :] = product
        partial_side[spot, :] = side

    def marks(n):
        return lax.broadcasted_iota(jnp.int32, (n * count, size), 0) % count

    def diagonal(values, spots):
        return jnp.concatenate(
            [jnp.where(spots == b, values, jnp.zeros_like(values)) for b in range(count)], axis=1
        )

    def rounded(v):
        return v.astype(jnp.bfloat16).astype(jnp.float32)

    mine = lax.broadcasted_iota(jnp.int32, rate_ref.shape, 1) == place
    rate = jnp.sum(jnp.where(mine, rate_ref[...], 0.0), axis=1, keepdims=True)

    def recall(c):
        main_copy(c).wait_recv()
        small_copy(c).wait_recv()
        begin = chip_of(c) * chip_rows
        whole = pl.ds(pl.multiple_of(begin, chip_rows), chip_rows)
        total = partial[whole, :] + received[c].astype(jnp.float32)
        flat = small_received[c].astype(jnp.float32)
        flat = jnp.concatenate([flat, jnp.zeros((128 - TINY, flat.shape[1]), jnp.float32)], axis=0)
        side = partial_side[whole, :] + flat.T[0:chip_rows]
        scale = lax.rsqrt(side[:, 2:3] / (cols * groups) + EPS)
        projected = rounded(total * scale)
        query = projected[:, :size]
        key = projected[:, size : 2 * size]
        query = query * lax.rsqrt(jnp.sum(query * query, axis=1, keepdims=True) + EPS) * size**-0.5
        key = key * lax.rsqrt(jnp.sum(key * key, axis=1, keepdims=True) + EPS)
        key_high, key_low = split(key)
        query_high, query_low = split(query)
        fetch(chip_of(c)).wait()
        spots = marks(4)
        for i in range(chip_rows // count):
            near = slice(i * count, (i + 1) * count)
            spot = pl.ds(pl.multiple_of(begin + i * count, count), count)
            four = [v[near] for v in (key_high, key_low, query_high, query_low)]
            wide = diagonal(jnp.concatenate(four, axis=0), spots)
            memory = held[spot].reshape(count * size, size).astype(jnp.bfloat16)
            both = jnp.dot(wide, memory, preferred_element_type=jnp.float32)
            answers[0, near, :] = both[0:count] + both[count : 2 * count]
            answers[1, near, :] = both[2 * count : 3 * count] + both[3 * count : 4 * count]
        pre = rounded(side * scale)
        strength = jax.nn.sigmoid(pre[:, 0:1])
        decay = pre[:, 1:2]
        softplus = jnp.maximum(decay, 0.0) + jnp.log(1.0 + jnp.exp(-jnp.abs(decay)))
        factor = jnp.broadcast_to(jnp.exp(-rate * softplus), (chip_rows, size))
        overlap = jnp.sum(query * key, axis=1, keepdims=True)
        gate = projected[:, 3 * size :]
        lift = head_gain_ref[...].astype(jnp.float32) * (gate / (1.0 + jnp.exp(-gate)))
        change = strength * (projected[:, 2 * size : 3 * size] - factor * answers[0])
        read = factor * answers[1] + overlap * change
        scaling = lax.rsqrt(jnp.sum(read * read, axis=1, keepdims=True) / size + EPS)
        gated[c] = (read * scaling * lift).astype(jnp.bfloat16)
        same = gated.at[c, pl.ds(pl.multiple_of(core * rows, rows), rows), :]
        cross = gated.at[c, pl.ds(pl.multiple_of((1 - core) * rows, rows), rows), :]
        for h in range(2 if c else 1):
            gap, row = (c // 2, c % 2) if h else (c % 2, c // 2)
            span = slice(row * rows, (row + 1) * rows)
            first = 2 * gap
            there = flip(partner, (h + 1,)) if gap else partner
            here = neighbours[h] if gap else me
            for source, phase, j, device in (
                (same, 1, first, there),
                (cross, 1, first + 1, flip(there, (0,))),
                (cross, 0, first + 1, flip(here, (0,))),
                (same, 0, first, here),
            ):
                target = left.at[h, phase, span, j * size : (j + 1) * size]
                if phase or j:
                    remote(source, target, send_sems.at[4], gated_recv.at[h, phase], device).start()
                else:
                    left[h, 0, span, 0:size] = gated[
                        c, pl.ds(pl.multiple_of(core * rows, rows), rows), :
                    ]
        kept = packed.at[c] if c < flats - 1 else late
        kept[0] = key
        kept[1] = change
        kept[2] = factor

    def update(c):
        begin = chip_of(c) * chip_rows

        def write(i, value):
            held[begin + i] = value

        renew(packed.at[c], lambda i: held[begin + i], write)

    def hop(phase, h, k):
        return remote(
            hop_out.at[phase, h, k],
            hop_in.at[phase, h, k],
            send_sems.at[5],
            hop_recv.at[phase, h, k],
            neighbours[1 - h],
        )

    slim = wide_half // 2

    def expand(phase):
        lefts = [left[0, phase], left[1, phase]]
        upper_rows = jnp.concatenate(
            [lefts[0][0:rows, 0 : 2 * size], lefts[1][0:rows, 2 * size :]], axis=1
        )
        lefts[1] = jnp.concatenate([upper_rows, lefts[1][rows:]], axis=0)
        for k in range(2):
            for h in range(2):
                begin = h * wide_half + k * slim
                span = slice(begin, begin + slim)
                product = lax.dot_general(
                    lefts[h],
                    four_w[span, :],
                    (((1,), (1,)), ((), ())),
                    preferred_element_type=jnp.float32,
                )
                hop_out[phase, h, k] = product[rows:].astype(jnp.bfloat16)
                hop(phase, h, k).start()
                acc[phase, :, span] = product[0:rows]

    def settle(phase):
        for k in range(2):
            for h in range(2):
                begin = h * wide_half + k * slim
                span = slice(begin, begin + slim)
                hop(phase, h, k).wait_recv()
                total = acc[phase, :, span] + hop_in[phase, h, k].astype(jnp.float32)

                @pl.when(keep == phase)
                def _():
                    mine_out[:, span] = total

                @pl.when(keep != phase)
                def _():
                    rise_out[:, span] = total.astype(jnp.bfloat16)

    def gated_bytes(h, phase):
        blocks = (6, 8) if h == 0 else (5, 6)
        return gathered.at[0:rows, 0 : blocks[phase] * size]

    def whole_left(phase):
        for h in range(2):
            target = gated_bytes(h, phase)
            remote(target, target, send_sems.at[4], gated_recv.at[h, phase], sibling).wait_recv()

    def relays(masks, halves=(0, 1)):
        for q in halves:
            for p, mask in masks:
                relay(p, q, mask)

    def send_beside(first, last):
        for i in range(first, last):
            for h in range(2):
                beside_w(h, i).start()

    def pass_weights(i):
        remote(*far_w(2 * tall), pair_sems.at[3], pair_sems.at[4 + i], sibling).wait_recv()
        for h in range(2):
            passed_w(h, i).start()

    def weights_ready():
        own_w.wait()
        sibling_w.wait_recv()
        remote(*far_w(cols), pair_sems.at[3], pair_sems.at[4 + pieces], sibling).wait_recv()

    def drain():
        sibling_w.wait_send()
        for i in range(2, 4):
            remote(*far_w(cols), pair_sems.at[i], pair_sems.at[4], sibling).wait_send()
        ici_rows = rows * (chips - 1)
        for i, ref in enumerate(
            (gathered.at[0:ici_rows, :], gathered.at[0 : rows * chips, :], sent, small_sent)
        ):
            remote(ref, ref, send_sems.at[i], main_recv.at[0], partner).wait_send()
        for phase in range(2):
            for h in range(2):
                target = gated_bytes(h, phase)
                remote(target, target, send_sems.at[4], gated_recv.at[0, 0], sibling).wait_send()
        remote(hop_out, hop_in, send_sems.at[5], hop_recv.at[0, 0, 0], sibling).wait_send()

    @pl.when(outer == 1)
    def _():
        relays([(0, z), (1, z)])
        project_away(0, 1)
        relays([(0, x + z), (1, y + z), (1, x + z), (0, y + z)])
        relays([(0, x), (1, y), (1, x), (0, y)])
        send_beside(0, pieces)
        project_away(1, 1)
        project_away(2, 1)
        project_here(0, 0)
        relays([(0, x + y + z), (1, x + y + z)])
        project_away(3, 1)
        relays([(0, x + y), (1, x + y)])
        project_here(1, 0)

    @pl.when(outer == 0)
    def _():
        project_away(0, 0, False)
        relays([(0, x), (1, y), (1, x), (0, y)], (0,))
        send_away(0)
        relays([(0, x), (1, y), (1, x), (0, y)], (1,))
        project_away(1, 0)
        project_away(2, 0)
        relays([(0, z), (1, z)])
        send_beside(0, 1)
        relays([(0, x + y), (1, x + y)])
        project_away(3, 0)
        relays([(0, x + z), (1, y + z), (1, x + z), (0, y + z)])
        send_beside(1, pieces)
        project_here(0, 1)
        relays([(0, x + y + z), (1, x + y + z)])
        project_here(1, 1)

    recall(0)
    recall(1)
    pass_weights(0)
    recall(2)
    pass_weights(1)
    pass_weights(2)
    pass_weights(3)
    recall(3)
    update(0)
    weights_ready()
    whole_left(0)
    expand(0)
    whole_left(1)
    expand(1)
    update(1)
    update(2)
    settle(0)
    settle(1)
    drain()


def fused(
    stream,
    norm_gain,
    weights,
    write_weight,
    decay_weight,
    rate,
    head_gain,
    out_weight,
    state,
    groups,
):
    rows, cols = stream.shape
    heads = rate.shape[0]
    size = weights[0].shape[1]
    chips = heads // 2
    flats = chips // 2
    batch = rows * heads
    chip_rows = 2 * rows
    dma = pltpu.SemaphoreType.DMA
    anywhere = pl.BlockSpec(memory_space=pltpu.HBM)
    f32, bf16 = jnp.float32, jnp.bfloat16
    return pl.pallas_call(
        functools.partial(fused_kernel, heads, groups),
        in_specs=[anywhere] * 12,
        out_specs=[VMEM] * 4,
        out_shape=[
            pltpu.VMEM(state.shape, state.dtype),
            pltpu.VMEM(stream.shape, f32),
            pltpu.VMEM(stream.shape, bf16),
            pltpu.VMEM((3, chip_rows, size), f32),
        ],
        scratch_shapes=[
            pltpu.VMEM(stream.shape, stream.dtype),
            pltpu.VMEM((groups * cols // 128, 128), bf16),
            pltpu.VMEM((1, heads), f32),
            pltpu.VMEM((1, size), bf16),
            pltpu.VMEM((batch, cols), bf16),
            pltpu.VMEM((cols, 4 * size), bf16),
            pltpu.VMEM((2 * heads, cols), bf16),
            pltpu.VMEM((2 * heads, cols), f32),
            pltpu.VMEM((2, cols), f32),
            pltpu.VMEM((1, cols), f32),
            pltpu.VMEM((groups * cols // 128, 128), f32),
            pltpu.VMEM((cols, 4 * size), bf16),
            pltpu.VMEM((flats * chip_rows, 4 * size), f32),
            pltpu.VMEM((flats * chip_rows, 128), f32),
            pltpu.VMEM((flats, chip_rows, 4 * size), bf16),
            pltpu.VMEM((flats, chip_rows, 4 * size), bf16),
            pltpu.VMEM((flats, TINY, max(128, chip_rows)), bf16),
            pltpu.VMEM((flats, TINY, max(128, chip_rows)), bf16),
            pltpu.VMEM((flats, 3, chip_rows, size), f32),
            pltpu.VMEM((2, chip_rows, size), f32),
            pltpu.VMEM((flats, chip_rows, size), bf16),
            pltpu.VMEM((2, 2, 2 * rows, 4 * size), bf16),
            pltpu.VMEM((2, rows, cols), f32),
            pltpu.VMEM((2, 2, 2, rows, cols // 4), bf16),
            pltpu.VMEM((2, 2, 2, rows, cols // 4), bf16),
            dma((7,)),
            dma((flats,)),
            dma((9,)),
            dma((6,)),
            dma((2, 2, chips - 1)),
            dma((chips,)),
            dma((flats,)),
            dma((flats,)),
            dma((2, 2)),
            dma((2, 2, 2)),
        ],
        compiler_params=pltpu.CompilerParams(
            collective_id=2, has_side_effects=True, vmem_limit_bytes=43 << 20
        ),
    )(
        stream,
        norm_gain.reshape(groups * cols // 128, 128),
        *weights,
        write_weight.T,
        decay_weight.T,
        rate.reshape(1, heads),
        head_gain.reshape(1, size),
        out_weight,
        state,
    )


def store_kernel(heads, held, late, new_ref, fresh, sems):
    place = lax.axis_index("tp") % heads
    count = late.shape[1]
    chunks = held.shape[0] // count
    last = chunks - 1 - place // 2 % chunks

    def copy(i, source):
        spot = pl.ds(pl.multiple_of((last + i) % chunks * count, count), count)
        origin = held.at[spot] if source is None else source
        return pltpu.make_async_copy(origin, new_ref.at[spot], sems.at[i])

    for i in range(1, chunks):
        copy(i, None).start()

    def write(i, value):
        fresh[i] = value

    renew(late, lambda i: held[last * count + i], write)
    copy(0, fresh).start()
    for i in range(1, chunks):
        copy(i, None).wait()
    copy(0, fresh).wait()


def store(held, late, heads):
    total, size, _ = held.shape
    count = late.shape[1]
    return pl.pallas_call(
        functools.partial(store_kernel, heads),
        in_specs=[VMEM] * 2,
        out_specs=pl.BlockSpec(memory_space=pl.ANY),
        out_shape=jax.ShapeDtypeStruct(held.shape, held.dtype),
        scratch_shapes=[
            pltpu.VMEM((count, size, size), held.dtype),
            pltpu.SemaphoreType.DMA((total // count,)),
        ],
        cost_estimate=pl.CostEstimate(
            flops=1000 * held.size, bytes_accessed=4 * held.size, transcendentals=0
        ),
        compiler_params=pltpu.CompilerParams(vmem_limit_bytes=10 << 20),
    )(held, late)


def per_device(
    stream,
    norm_gain,
    query_weight,
    key_weight,
    value_weight,
    gate_weight,
    write_weight,
    decay_weight,
    decay_rate,
    head_gain,
    out_weight,
    state,
):
    heads = decay_rate.shape[0]
    groups = lax.axis_size("tp") // heads
    weights = (query_weight, key_weight, value_weight, gate_weight)
    rows, cols = stream.shape
    if groups == 2 and heads == 16 and rows % 32 == 0 and rows <= 64 and cols % 256 == 0:
        held, mine, rise, late = fused(
            stream,
            norm_gain,
            weights,
            write_weight,
            decay_weight,
            decay_rate,
            head_gain,
            out_weight,
            state,
            groups,
        )
        span = heads // 2
        pairs = [
            (i, i + span * (1 - 2 * (i // span % 2))) for i in range(lax.axis_size("tp"))
        ]
        arrived = lax.ppermute(rise, "tp", pairs)
        updated = store(held, late, heads)
        result = stream.astype(jnp.float32) + mine + arrived.astype(jnp.float32)
        return (result.astype(stream.dtype), updated)
    packed = project(
        stream, norm_gain, weights, write_weight, decay_weight, decay_rate, heads, groups
    )
    updated, gated, scaling = state_step(state, packed, head_gain)
    result = output(stream, gated, scaling, out_weight, heads, groups)
    return (result, updated)


def solution(mesh):
    placed = (
        P("tp", None),
        P(),
        P("tp", None),
        P("tp", None),
        P("tp", None),
        P("tp", None),
        P(),
        P(),
        P(),
        P(),
        P("tp", None),
        P("tp", None, None),
    )
    return jax.shard_map(
        per_device,
        mesh=mesh,
        in_specs=placed,
        out_specs=(P("tp", None), P("tp", None, None)),
        check_vma=False,
    )
```
